32 devices in a mesh: sp: 8 (over z, x), tp: 4 (over y, core).
Axes of the slice: x: 2, y: 2, z: 4, core: 2. Of those that a mesh axis runs over, the one named last changes fastest.
Arguments:
- residual: bfloat16 [8192, 2048], P('sp'), may hold values from -6 to 6
- query: bfloat16 [8192, 1024], P('sp', 'tp'), may hold values from -6 to 6
- key: bfloat16 [8192, 256], P('sp', 'tp'), may hold values from -6 to 6
- value: bfloat16 [8192, 256], P('sp', 'tp'), may hold values from -6 to 6
- sink: float32 [16], P('tp'), may hold values from 3 to 9
- norm_gain: float32 [2048], replicated, may hold values from 0.1 to 1.9
- w_out: bfloat16 [1024, 2048], P('tp'), may hold values from -1.5 to 1.5
- w_gate: bfloat16 [2048, 4096], P('sp', 'tp'), may hold values from -0.125 to 0.125
- w_value: bfloat16 [2048, 4096], P('sp', 'tp'), may hold values from -0.125 to 0.125
- conv_gate: bfloat16 [3, 4096], P(None, 'tp'), may hold values from -3 to 3
- conv_value: bfloat16 [3, 4096], P(None, 'tp'), may hold values from -3 to 3
- w_down: bfloat16 [4096, 2048], P('tp', 'sp'), may hold values from -0.09375 to 0.09375
Outputs:
- layer_out: bfloat16 [8192, 2048], P(('sp', 'tp'))
The draws below stay inside these ranges and needn't reach their ends.
All inputs are finite; a program needn't handle non-finite values.
Results may differ from the reference program's by a relative error of at most 0.015.
Values may be sent and summed in bfloat16 or wider, within the bound.
A program may use at most 128 MiB of HBM per device.

```python
import jax
import jax.numpy as jnp
from jax import lax

D = 2048
FF = 4096
HEADS = 16
KV_HEADS = 4
HD = 64
WINDOW = 128
TOKENS = 8192
N_TP = 4


def draw_key(key, part):
    base = jax.random.fold_in(key, 11)
    shape = (TOKENS, KV_HEADS * HD)
    return jnp.clip(jax.random.normal(jax.random.fold_in(base, 1), shape, jnp.float32), -6.0, 6.0).astype(jnp.bfloat16)


def draw_query(key, part):
    base = jax.random.fold_in(key, 11)
    shape = (TOKENS, HEADS * HD)
    return jnp.clip(jax.random.normal(jax.random.fold_in(base, 2), shape, jnp.float32), -6.0, 6.0).astype(jnp.bfloat16)


def steps_of(key, shape, split, smallest, top_value):
    level = 1.0
    for dim, shards_of in split:
        heights = jax.random.uniform(jax.random.fold_in(jax.random.fold_in(key, 6), dim), (shards_of,), jnp.float32, smallest / len(split), top_value / len(split))
        level = level * jnp.repeat(jnp.exp(heights), shape[dim] // shards_of).reshape((-1,) + (1,) * (len(shape) - 1 - dim))
    return level


def bell_draw(stream_key, dims, scale, most, shards=(), held_as=jnp.bfloat16):
    level = steps_of(stream_key, dims, shards, -0.22, 0.18) if shards else 1.0
    array = jax.random.normal(stream_key, dims, jnp.float32) * scale * level
    return jnp.minimum(jnp.maximum(array, -most), most).astype(held_as)


def setup_inputs(seed: int = 0) -> dict:
    key_of = jax.random.split(jax.random.key(seed), 13)
    residual = bell_draw(key_of[0], (TOKENS, D), 1.0, 6.0, ((0, 8),))
    query = draw_query(jax.random.fold_in(key_of[12], 71), 0)
    key = draw_key(jax.random.fold_in(key_of[12], 71), 0)
    value = bell_draw(key_of[3], (TOKENS, KV_HEADS * HD), 1.0, 6.0, ((0, 8), (1, 4)))
    sink = jnp.clip(3.0 + 6.0 * jax.random.uniform(key_of[4], (HEADS,), jnp.float32) ** steps_of(key_of[4], (HEADS,), ((0, 4),), -0.2, 0.2), 3.0, 9.0)
    norm_gain = jnp.clip(1.0 + 0.18 * jax.random.normal(key_of[5], (D,), jnp.float32), 0.1, 1.9)
    w_out = bell_draw(key_of[6], (HEADS * HD, D), (HD // 4) ** -0.5, 1.5, ((0, 4),))
    w_gate = bell_draw(key_of[7], (D, FF), D ** -0.5, 0.125, ((0, 8), (1, 4)))
    w_value = bell_draw(key_of[8], (D, FF), D ** -0.5, 0.125, ((0, 8), (1, 4)))
    conv_gate = bell_draw(key_of[9], (3, FF), 0.577, 3.0, ((1, 4),))
    conv_value = bell_draw(key_of[10], (3, FF), 0.577, 3.0, ((1, 4),))
    w_down = bell_draw(key_of[11], (FF, D), FF ** -0.5, 0.09375, ((0, 4), (1, 8)))
    return {"residual": residual, "query": query, "key": key, "value": value, "sink": sink, "norm_gain": norm_gain, "w_out": w_out, "w_gate": w_gate, "w_value": w_value, "conv_gate": conv_gate, "conv_value": conv_value, "w_down": w_down}


THETA = 10000.0
EPS = 1e-06

def rotate(field, positions):
    count = field.shape[0]
    parts = field.astype(jnp.float32).reshape(count, -1, HD)
    inverse = 1.0 / THETA ** (jnp.arange(0, HD, 2, dtype=jnp.float32) / HD)
    angle = positions[:, None] * inverse[None, :]
    cosine = jnp.cos(angle)[:, None, :]
    sine = jnp.sin(angle)[:, None, :]
    first = parts[..., :HD // 2]
    second = parts[..., HD // 2:]
    turned = jnp.concatenate([first * cosine - second * sine, second * cosine + first * sine], axis=-1)
    return turned.reshape(count, -1).astype(jnp.bfloat16)

def band_attention(queries, keys, values, sinks, start, total):
    count = queries.shape[0]
    blocks = count // WINDOW
    kv_local = keys.shape[1] // HD
    group = queries.shape[1] // (kv_local * HD)
    query_blocks = queries.astype(jnp.float32).reshape(blocks, WINDOW, kv_local, group, HD)
    key_band = jnp.concatenate([keys[i * WINDOW:i * WINDOW + count].reshape(blocks, WINDOW, kv_local, HD) for i in range(3)], axis=1).astype(jnp.float32)
    value_band = jnp.concatenate([values[i * WINDOW:i * WINDOW + count].reshape(blocks, WINDOW, kv_local, HD) for i in range(3)], axis=1).astype(jnp.float32)
    scores = jnp.einsum('nqkgd,njkd->nkgqj', query_blocks, key_band) * HD ** (-0.5)
    block_ids = jnp.arange(blocks, dtype=jnp.int32)[:, None]
    query_pos = start + block_ids * WINDOW + jnp.arange(WINDOW, dtype=jnp.int32)[None, :]
    key_pos = start - WINDOW + block_ids * WINDOW + jnp.arange(3 * WINDOW, dtype=jnp.int32)[None, :]
    valid = (key_pos[:, None, :] >= 0) & (key_pos[:, None, :] < total) & (jnp.abs(query_pos[:, :, None] - key_pos[:, None, :]) <= WINDOW)
    scores = jnp.where(valid[:, None, None], scores, -1e+30)
    sink_col = sinks.astype(jnp.float32).reshape(1, kv_local, group, 1, 1)
    top = jnp.maximum(lax.optimization_barrier(jnp.max(scores, axis=-1, keepdims=True)), sink_col)
    weights = jnp.exp(scores - top)
    denom = lax.optimization_barrier(jnp.sum(weights, axis=-1, keepdims=True)) + jnp.exp(sink_col - top)
    probs = (weights / denom).astype(jnp.bfloat16)
    out = jnp.einsum('nkgqj,njkd->nqkgd', probs.astype(jnp.float32), value_band)
    return out.reshape(count, kv_local * group * HD).astype(jnp.bfloat16)

def rmsnorm(field, gain):
    wide = field.astype(jnp.float32)
    scale = lax.rsqrt(lax.optimization_barrier(jnp.mean(wide * wide, axis=-1, keepdims=True)) + EPS)
    return (wide * scale * gain).astype(jnp.bfloat16)

def block_sum(left, right, pieces):
    width = left.shape[1] // pieces
    summed = jnp.zeros((left.shape[0], right.shape[1]), jnp.float32)
    for index in range(pieces):
        term = jnp.dot(left[:, index * width:(index + 1) * width], right[index * width:(index + 1) * width], preferred_element_type=jnp.float32)
        rounded = lax.optimization_barrier(term.astype(jnp.bfloat16))
        summed = summed + rounded.astype(jnp.float32)
    return summed

def reference(residual, query, key, value, sink, norm_gain, w_out, w_gate, w_value, conv_gate, conv_value, w_down):
    total = query.shape[0]
    kv_heads = key.shape[1] // HD
    group = query.shape[1] // key.shape[1]
    positions = jnp.arange(total, dtype=jnp.float32)
    turned_query = rotate(query, positions)
    turned_key = rotate(key, positions)
    pad = ((WINDOW, WINDOW), (0, 0))
    keys_ext = jnp.pad(turned_key, pad)
    values_ext = jnp.pad(value, pad)
    query_heads = turned_query.reshape(total, kv_heads, group * HD).transpose(1, 0, 2)
    key_heads = keys_ext.reshape(total + 2 * WINDOW, kv_heads, HD).transpose(1, 0, 2)
    value_heads = values_ext.reshape(total + 2 * WINDOW, kv_heads, HD).transpose(1, 0, 2)
    sink_heads = sink.reshape(kv_heads, group)

    def one_head(args):
        return band_attention(args[0], args[1], args[2], args[3], 0, total)
    outs = lax.map(one_head, (query_heads, key_heads, value_heads, sink_heads))
    attended = outs.transpose(1, 0, 2).reshape(total, -1)
    mix = block_sum(attended, w_out, N_TP)
    mid = (residual.astype(jnp.float32) + mix).astype(jnp.bfloat16)
    normed = rmsnorm(mid, norm_gain)
    gate_up = jnp.dot(normed, w_gate, preferred_element_type=jnp.float32).astype(jnp.bfloat16)
    value_up = jnp.dot(normed, w_value, preferred_element_type=jnp.float32).astype(jnp.bfloat16)

    def convolve(field, taps):
        padded = jnp.pad(field, ((1, 1), (0, 0))).astype(jnp.float32)
        taps = taps.astype(jnp.float32)
        return padded[:-2] * taps[0] + padded[1:-1] * taps[1] + padded[2:] * taps[2]
    gate_conv = convolve(gate_up, conv_gate)
    value_conv = convolve(value_up, conv_value)
    hidden = (jax.nn.silu(gate_conv) * value_conv).astype(jnp.bfloat16)
    ffn = block_sum(hidden, w_down, N_TP)
    return (mid.astype(jnp.float32) + ffn).astype(jnp.bfloat16)
```

```python
import jax
import jax.numpy as jnp
from jax import lax
from jax.sharding import PartitionSpec as P

HD = 64
WINDOW = 128


THETA = 10000.0
EPS = 1e-06


def extended(block, sides, width):
    for axis, dim in sides:
        count = lax.axis_size(axis)
        forward = [(i, i + 1) for i in range(count - 1)]
        backward = [(target, source) for source, target in forward]
        low = lax.ppermute(
            lax.slice_in_dim(block, block.shape[dim] - width, None, axis=dim), axis, forward
        )
        high = lax.ppermute(lax.slice_in_dim(block, 0, width, axis=dim), axis, backward)
        block = jnp.concatenate([low, block, high], axis=dim)
    return block


def rotate(field, positions):
    count = field.shape[0]
    parts = field.astype(jnp.float32).reshape(count, -1, HD)
    inverse = 1.0 / THETA ** (jnp.arange(0, HD, 2, dtype=jnp.float32) / HD)
    angle = positions[:, None] * inverse[None, :]
    cosine = jnp.cos(angle)[:, None, :]
    sine = jnp.sin(angle)[:, None, :]
    first = parts[..., : HD // 2]
    second = parts[..., HD // 2 :]
    turned = jnp.concatenate(
        [first * cosine - second * sine, second * cosine + first * sine], axis=-1
    )
    return turned.reshape(count, -1).astype(jnp.bfloat16)


def band_attention(queries, keys, values, sinks, start, total):
    count = queries.shape[0]
    blocks = count // WINDOW
    kv_local = keys.shape[1] // HD
    group = queries.shape[1] // (kv_local * HD)
    query_blocks = queries.reshape(blocks, WINDOW, kv_local, group, HD)
    key_band = jnp.concatenate(
        [
            keys[i * WINDOW : i * WINDOW + count].reshape(blocks, WINDOW, kv_local, HD)
            for i in range(3)
        ],
        axis=1,
    )
    value_band = jnp.concatenate(
        [
            values[i * WINDOW : i * WINDOW + count].reshape(blocks, WINDOW, kv_local, HD)
            for i in range(3)
        ],
        axis=1,
    )
    scores = jnp.einsum(
        "nqkgd,njkd->nkgqj", query_blocks, key_band, preferred_element_type=jnp.float32
    ) * HD ** (-0.5)
    block_ids = jnp.arange(blocks, dtype=jnp.int32)[:, None]
    query_pos = start + block_ids * WINDOW + jnp.arange(WINDOW, dtype=jnp.int32)[None, :]
    key_pos = start - WINDOW + block_ids * WINDOW + jnp.arange(3 * WINDOW, dtype=jnp.int32)[None, :]
    valid = (
        (key_pos[:, None, :] >= 0)
        & (key_pos[:, None, :] < total)
        & (jnp.abs(query_pos[:, :, None] - key_pos[:, None, :]) <= WINDOW)
    )
    scores = jnp.where(valid[:, None, None], scores, -1e30)
    sink_col = sinks.reshape(1, kv_local, group, 1, 1)
    top = jnp.maximum(jnp.max(scores, axis=-1, keepdims=True), sink_col)
    weights = jnp.exp(scores - top)
    denom = jnp.sum(weights, axis=-1, keepdims=True) + jnp.exp(sink_col - top)
    probs = (weights / denom).astype(jnp.bfloat16)
    out = jnp.einsum("nkgqj,njkd->nqkgd", probs, value_band, preferred_element_type=jnp.float32)
    return out.reshape(count, kv_local * group * HD).astype(jnp.bfloat16)


def rmsnorm(field, gain):
    wide = field.astype(jnp.float32)
    scale = lax.rsqrt(jnp.mean(wide * wide, axis=-1, keepdims=True) + EPS)
    return (wide * scale * gain).astype(jnp.bfloat16)


def swap(field, axis, distance):
    count = lax.axis_size(axis)
    return lax.ppermute(field, axis, [(i, i ^ distance) for i in range(count)])


def gathered(block, axis, pair):
    count = lax.axis_size(axis)
    index = lax.axis_index(axis)
    line = count // pair
    place = index // pair
    up = [(i, i + pair) for i in range(count - pair)]
    down = [(j, i) for i, j in up]
    ups, downs = [block], [block]
    for _ in range(line - 1):
        ups.append(lax.ppermute(ups[-1], axis, up))
        downs.append(lax.ppermute(downs[-1], axis, down))
    column = [block]
    for k in range(1, line):
        column.append(jnp.where(place >= k, ups[k], downs[line - k]))
    out = jnp.zeros((count,) + block.shape, block.dtype)
    for k in range(line):
        source = (place - k) % line
        for other in range(pair):
            piece = column[k] if other == 0 else swap(column[k], axis, other)
            out = lax.dynamic_update_slice_in_dim(
                out, piece[None], source * pair + (index % pair ^ other), 0
            )
    return out


def over_tp(block):
    count = lax.axis_size("tp")
    blocks = [block]
    step = count // 2
    while step:
        blocks = blocks + [swap(b, "tp", step) for b in blocks]
        step //= 2
    return blocks


def shards(
    residual,
    query,
    key,
    value,
    sink,
    norm_gain,
    w_out,
    w_gate,
    w_value,
    conv_gate,
    conv_value,
    w_down,
):
    tok_rows = query.shape[0]
    offset = lax.axis_index("sp") * tok_rows
    total = tok_rows * lax.axis_size("sp")
    share = tok_rows // lax.axis_size("tp")
    tp_index = lax.axis_index("tp")
    positions = (offset + jnp.arange(tok_rows, dtype=jnp.int32)).astype(jnp.float32)
    turned_query = rotate(query, positions)
    turned_key = rotate(key, positions)
    key_width = key.shape[1]
    band = jnp.concatenate([turned_key, value], axis=1)
    edged = extended(band, (("sp", 0),), WINDOW)
    out_blocks = over_tp(w_out)
    hidden_width = w_gate.shape[1]
    up_full = gathered(jnp.concatenate([w_gate, w_value], axis=1), "sp", 2)
    up_full = up_full.reshape(-1, 2 * hidden_width)
    attended = band_attention(
        turned_query, edged[:, :key_width], edged[:, key_width:], sink, offset, total
    )
    att_blocks = over_tp(attended)
    mix_full = sum(
        jnp.dot(a, w, preferred_element_type=jnp.float32).astype(jnp.bfloat16).astype(jnp.float32)
        for a, w in zip(att_blocks, out_blocks)
    )
    mid_full = (residual.astype(jnp.float32) + mix_full).astype(jnp.bfloat16)
    normed = rmsnorm(mid_full, norm_gain)
    mid_rows = lax.dynamic_slice_in_dim(mid_full, tp_index * share, share, 0)
    stacked = jnp.dot(normed, up_full, preferred_element_type=jnp.float32).astype(jnp.bfloat16)
    edged_up = extended(stacked, (("sp", 0),), 1).astype(jnp.float32)
    taps = jnp.concatenate([conv_gate, conv_value], axis=1).astype(jnp.float32)
    convolved = edged_up[:-2] * taps[0] + edged_up[1:-1] * taps[1] + edged_up[2:] * taps[2]
    hidden = (jax.nn.silu(convolved[:, :hidden_width]) * convolved[:, hidden_width:]).astype(
        jnp.bfloat16
    )
    down_full = gathered(w_down, "sp", 2)
    terms = jnp.einsum("th,nhc->tnc", hidden, down_full, preferred_element_type=jnp.float32)
    terms = terms.reshape(tok_rows, -1)
    ffn_rows = lax.psum_scatter(
        terms.astype(jnp.bfloat16), "tp", scatter_dimension=0, tiled=True
    ).astype(jnp.float32)
    return (mid_rows.astype(jnp.float32) + ffn_rows).astype(jnp.bfloat16)


def solution(mesh):
    return jax.shard_map(
        shards,
        mesh=mesh,
        in_specs=(
            P("sp", None),
            P("sp", "tp"),
            P("sp", "tp"),
            P("sp", "tp"),
            P("tp"),
            P(),
            P("tp", None),
            P("sp", "tp"),
            P("sp", "tp"),
            P(None, "tp"),
            P(None, "tp"),
            P("tp", "sp"),
        ),
        out_specs=P(("sp", "tp"), None),
        check_vma=False,
    )
```

```python
import functools

import jax
import jax.numpy as jnp
from jax import lax
from jax.experimental import pallas as pl
from jax.experimental.pallas import tpu as pltpu
from jax.sharding import PartitionSpec as P

HD = 64
WINDOW = 128


THETA = 10000.0
EPS = 1e-06


def extended(block, sides, width):
    for axis, dim in sides:
        count = lax.axis_size(axis)
        forward = [(i, i + 1) for i in range(count - 1)]
        backward = [(target, source) for source, target in forward]
        low = lax.ppermute(
            lax.slice_in_dim(block, block.shape[dim] - width, None, axis=dim), axis, forward
        )
        high = lax.ppermute(lax.slice_in_dim(block, 0, width, axis=dim), axis, backward)
        block = jnp.concatenate([low, block, high], axis=dim)
    return block


def rotate(field, positions):
    count = field.shape[0]
    parts = field.astype(jnp.float32).reshape(count, -1, HD)
    inverse = 1.0 / THETA ** (jnp.arange(0, HD, 2, dtype=jnp.float32) / HD)
    angle = positions[:, None] * inverse[None, :]
    cosine = jnp.cos(angle)[:, None, :]
    sine = jnp.sin(angle)[:, None, :]
    first = parts[..., : HD // 2]
    second = parts[..., HD // 2 :]
    turned = jnp.concatenate(
        [first * cosine - second * sine, second * cosine + first * sine], axis=-1
    )
    return turned.reshape(count, -1).astype(jnp.bfloat16)


def band_attention(queries, keys, values, sinks, start, total):
    count = queries.shape[0]
    blocks = count // WINDOW
    kv_local = keys.shape[1] // HD
    group = queries.shape[1] // (kv_local * HD)
    query_blocks = queries.reshape(blocks, WINDOW, kv_local, group, HD)
    key_band = jnp.concatenate(
        [
            keys[i * WINDOW : i * WINDOW + count].reshape(blocks, WINDOW, kv_local, HD)
            for i in range(3)
        ],
        axis=1,
    )
    value_band = jnp.concatenate(
        [
            values[i * WINDOW : i * WINDOW + count].reshape(blocks, WINDOW, kv_local, HD)
            for i in range(3)
        ],
        axis=1,
    )
    scores = jnp.einsum(
        "nqkgd,njkd->nkgqj", query_blocks, key_band, preferred_element_type=jnp.float32
    ) * HD ** (-0.5)
    block_ids = jnp.arange(blocks, dtype=jnp.int32)[:, None]
    query_pos = start + block_ids * WINDOW + jnp.arange(WINDOW, dtype=jnp.int32)[None, :]
    key_pos = start - WINDOW + block_ids * WINDOW + jnp.arange(3 * WINDOW, dtype=jnp.int32)[None, :]
    valid = (
        (key_pos[:, None, :] >= 0)
        & (key_pos[:, None, :] < total)
        & (jnp.abs(query_pos[:, :, None] - key_pos[:, None, :]) <= WINDOW)
    )
    scores = jnp.where(valid[:, None, None], scores, -1e30)
    sink_col = sinks.reshape(1, kv_local, group, 1, 1)
    top = jnp.maximum(jnp.max(scores, axis=-1, keepdims=True), sink_col)
    weights = jnp.exp(scores - top)
    denom = jnp.sum(weights, axis=-1, keepdims=True) + jnp.exp(sink_col - top)
    probs = (weights / denom).astype(jnp.bfloat16)
    out = jnp.einsum("nkgqj,njkd->nqkgd", probs, value_band, preferred_element_type=jnp.float32)
    return out.reshape(count, kv_local * group * HD).astype(jnp.bfloat16)


def rmsnorm(field, gain):
    wide = field.astype(jnp.float32)
    scale = lax.rsqrt(jnp.mean(wide * wide, axis=-1, keepdims=True) + EPS)
    return (wide * scale * gain).astype(jnp.bfloat16)


def plain_shards(
    residual,
    query,
    key,
    value,
    sink,
    norm_gain,
    w_out,
    w_gate,
    w_value,
    conv_gate,
    conv_value,
    w_down,
):
    tok_rows = query.shape[0]
    offset = lax.axis_index("sp") * tok_rows
    total = tok_rows * lax.axis_size("sp")
    share = tok_rows // lax.axis_size("tp")
    tp_index = lax.axis_index("tp")
    positions = (offset + jnp.arange(tok_rows, dtype=jnp.int32)).astype(jnp.float32)
    turned_query = rotate(query, positions)
    turned_key = rotate(key, positions)
    key_width = key.shape[1]
    band = jnp.concatenate([turned_key, value], axis=1)
    edged = extended(band, (("sp", 0),), WINDOW)
    attended = band_attention(
        turned_query, edged[:, :key_width], edged[:, key_width:], sink, offset, total
    )
    partial_value = jnp.dot(attended, w_out, preferred_element_type=jnp.float32)
    mix_full = lax.psum(partial_value.astype(jnp.bfloat16), "tp").astype(jnp.float32)
    mid_full = (residual.astype(jnp.float32) + mix_full).astype(jnp.bfloat16)
    normed = rmsnorm(mid_full, norm_gain)
    mid_rows = lax.dynamic_slice_in_dim(mid_full, tp_index * share, share, 0)
    gate_full, value_full = (
        lax.all_gather(w_gate, "sp", axis=0, tiled=True),
        lax.all_gather(w_value, "sp", axis=0, tiled=True),
    )
    gate_up = jnp.dot(normed, gate_full, preferred_element_type=jnp.float32).astype(jnp.bfloat16)
    value_up = jnp.dot(normed, value_full, preferred_element_type=jnp.float32).astype(jnp.bfloat16)
    hidden_width = gate_up.shape[1]
    stacked = jnp.concatenate([gate_up, value_up], axis=1)
    edged_up = extended(stacked, (("sp", 0),), 1).astype(jnp.float32)
    taps = jnp.concatenate([conv_gate, conv_value], axis=1).astype(jnp.float32)
    convolved = edged_up[:-2] * taps[0] + edged_up[1:-1] * taps[1] + edged_up[2:] * taps[2]
    hidden = (jax.nn.silu(convolved[:, :hidden_width]) * convolved[:, hidden_width:]).astype(
        jnp.bfloat16
    )
    terms = jnp.dot(
        hidden, lax.all_gather(w_down, "sp", axis=1, tiled=True), preferred_element_type=jnp.float32
    )
    ffn_rows = lax.psum_scatter(
        terms.astype(jnp.bfloat16), "tp", scatter_dimension=0, tiled=True
    ).astype(jnp.float32)
    return (mid_rows.astype(jnp.float32) + ffn_rows).astype(jnp.bfloat16)


F32 = jnp.float32
BF16 = jnp.bfloat16
PAIR = 2
EDGE = 8


def layer_kernel(
    sp,
    tp,
    q_ref,
    band_ref,
    sink_ref,
    res_ref,
    gain_ref,
    wo_ref,
    wg_ref,
    wv_ref,
    tg_ref,
    tv_ref,
    wd_ref,
    out_ref,
    band,
    att,
    wo,
    wg,
    wv,
    wd,
    mid,
    normed,
    upg,
    upv,
    hidden,
    terms,
    rbuf,
    local_sem,
    up_send,
    up_recv,
    dn_send,
    dn_recv,
    wo_send,
    wo_recv,
    att_send,
    att_recv,
    kv_send,
    kv_recv,
    edge_send,
    edge_recv,
    rs_send,
    rs_recv,
):
    me = lax.axis_index("sp")
    my_tp = lax.axis_index("tp")
    tok = res_ref.shape[0]
    width = res_ref.shape[1]
    share = tok // tp
    line = sp // PAIR
    place = me // PAIR
    side = me % PAIR
    mate = place * PAIR + (1 - side)
    depth = wg_ref.shape[0]
    cols = wd_ref.shape[1]
    hid = wg_ref.shape[1]
    has_low = me > 0
    has_high = me < sp - 1
    can_down = place > 0
    can_up = place < line - 1
    peers = [lax.rem(my_tp + k, tp) for k in range(1, tp)]

    def remote(src, dst, send, recv, **where):
        return pltpu.make_async_remote_copy(
            src_ref=src,
            dst_ref=dst,
            send_sem=send,
            recv_sem=recv,
            device_id=where,
            device_id_type=pl.DeviceIdType.MESH,
        )

    barrier = pltpu.get_barrier_semaphore()

    def greet(**where):
        pl.semaphore_signal(
            barrier, inc=1, device_id=where, device_id_type=pl.DeviceIdType.MESH
        )

    greet(sp=mate)
    for peer in peers:
        greet(tp=peer)
    far_low = has_low & (side == 0)
    far_high = has_high & (side == PAIR - 1)
    pl.when(far_low)(lambda: greet(sp=me - 1))
    pl.when(far_high)(lambda: greet(sp=me + 1))
    pl.when(can_down)(lambda: greet(sp=me - PAIR))
    pl.when(can_up)(lambda: greet(sp=me + PAIR))
    count = tp
    for able in (far_low, far_high, can_down, can_up):
        count = count + jnp.where(able, 1, 0)
    pl.semaphore_wait(barrier, count)

    def up_slot(kind, block):
        return (wg, wv)[kind].at[pl.ds(pl.multiple_of(block * depth, depth), depth), :]

    def up_copy(kind, block, way, own=False):
        target = (me - PAIR, me + PAIR, mate)[way]
        slot = up_slot(kind, block)
        return remote(
            (wg_ref, wv_ref)[kind] if own else slot,
            slot,
            up_send.at[kind, block, way],
            up_recv.at[kind, block],
            sp=target,
        )

    def dn_copy(block, way, own=False):
        target = (me - PAIR, me + PAIR, mate)[way]
        slot = wd.at[block]
        return remote(
            wd_ref if own else slot, slot, dn_send.at[block, way], dn_recv.at[block], sp=target
        )

    def candidate(c):
        distance = (c + 1) // 2
        there = jnp.where(c % 2 == 1, place + distance, place - distance)
        valid = (there >= 0) & (there < line)
        above = there > place
        return there, valid, above

    own_local = [
        pltpu.make_async_copy(wg_ref, up_slot(0, me), local_sem.at[0]),
        pltpu.make_async_copy(wv_ref, up_slot(1, me), local_sem.at[1]),
        pltpu.make_async_copy(wd_ref, wd.at[me], local_sem.at[2]),
        pltpu.make_async_copy(wo_ref, wo.at[my_tp], local_sem.at[3]),
        pltpu.make_async_copy(band_ref, band.at[pl.ds(WINDOW, tok), :], local_sem.at[4]),
    ]

    kv_low = remote(
        band_ref.at[pl.ds(0, WINDOW), :],
        band.at[pl.ds(WINDOW + tok, WINDOW), :],
        kv_send.at[0],
        kv_recv.at[1],
        sp=me - 1,
    )
    kv_high = remote(
        band_ref.at[pl.ds(tok - WINDOW, WINDOW), :],
        band.at[pl.ds(0, WINDOW), :],
        kv_send.at[1],
        kv_recv.at[0],
        sp=me + 1,
    )
    pl.when(has_low)(kv_low.start)
    pl.when(has_high)(kv_high.start)
    for copy in own_local:
        copy.start()
    for kind in range(2):
        up_copy(kind, me, 2, True).start()
        pl.when(can_down)(up_copy(kind, me, 0, True).start)
        pl.when(can_up)(up_copy(kind, me, 1, True).start)

    def wo_copy(k):
        return remote(wo_ref, wo.at[my_tp], wo_send.at[k], wo_recv.at[my_tp], tp=peers[k])

    for k in range(tp - 1):
        wo_copy(k).start()

    blank = jnp.zeros((WINDOW, band.shape[1]), BF16)

    @pl.when(jnp.logical_not(has_low))
    def _():
        band[pl.ds(0, WINDOW), :] = blank

    @pl.when(jnp.logical_not(has_high))
    def _():
        band[pl.ds(WINDOW + tok, WINDOW), :] = blank

    own_local[4].wait()
    pl.when(has_low)(kv_high.wait_recv)
    pl.when(has_high)(kv_low.wait_recv)
    heads = q_ref.shape[0]
    span = 3 * WINDOW
    total = tok * sp

    def attend(i, carry):
        start = pl.multiple_of(i * WINDOW, WINDOW)
        keys = band[pl.ds(start, span), :]
        row = lax.broadcasted_iota(jnp.int32, (WINDOW, span), 0)
        col = lax.broadcasted_iota(jnp.int32, (WINDOW, span), 1)
        key_pos = col + (me * tok - WINDOW + start)
        valid = (col >= row) & (col <= row + 2 * WINDOW) & (key_pos >= 0) & (key_pos < total)
        lane = lax.broadcasted_iota(jnp.int32, (WINDOW, 2 * HD), 1)
        outs = []
        for h in range(heads):
            scores = lax.dot_general(
                q_ref[h, pl.ds(start, WINDOW), :],
                keys,
                (((1,), (1,)), ((), ())),
                preferred_element_type=F32,
            )
            scores = jnp.where(valid, scores, -1e30)
            sink = sink_ref[h]
            top = jnp.maximum(jnp.max(scores, axis=-1, keepdims=True), sink)
            weights = jnp.exp(scores - top)
            denom = jnp.sum(weights, axis=-1, keepdims=True) + jnp.exp(sink - top)
            probs = (weights * (1.0 / denom)).astype(BF16)
            outs.append(jnp.dot(probs, keys, preferred_element_type=F32))
        for h in range(0, heads, 2):
            pair = jnp.where(lane < HD, pltpu.roll(outs[h], HD, 1), outs[h + 1])
            att[my_tp, pl.ds(start, WINDOW), pl.ds(h * HD, 2 * HD)] = pair.astype(BF16)
        return carry

    lax.fori_loop(0, tok // WINDOW, attend, 0)

    def att_copy(k):
        return remote(
            att.at[my_tp], att.at[my_tp], att_send.at[k], att_recv.at[my_tp], tp=peers[k]
        )

    for k in range(tp - 1):
        att_copy(k).start()

    def pass_up(c, carry):
        there, valid, above = candidate(c)
        block = there * PAIR + side

        @pl.when(valid)
        def _():
            for kind in range(2):
                up_copy(kind, block, 2).wait_recv()
                up_copy(kind, block, 2).start()
                pl.when(above & can_down)(up_copy(kind, block, 0).start)
                pl.when(jnp.logical_not(above) & can_up)(up_copy(kind, block, 1).start)

        return carry

    def start_down():
        dn_copy(me, 2, True).start()
        pl.when(can_down)(dn_copy(me, 0, True).start)
        pl.when(can_up)(dn_copy(me, 1, True).start)

    lax.fori_loop(1, 2 * line - 1, pass_up, 0)
    start_down()

    own_local[3].wait()
    for k in range(tp - 1):
        src = peers[k]
        remote(wo_ref, wo.at[src], wo_send.at[k], wo_recv.at[src], tp=src).wait_recv()
        remote(att.at[src], att.at[src], att_send.at[k], att_recv.at[src], tp=src).wait_recv()
    tile = tok // 4
    piece = 512

    def mix(i, carry):
        rows = pl.ds(pl.multiple_of(i * tile, tile), tile)
        squares = jnp.zeros((tile, 1), F32)
        for c in range(0, width, piece):
            acc = jnp.zeros((tile, piece), F32)
            for k in range(tp):
                term = jnp.dot(
                    att[k, rows, :], wo[k, :, pl.ds(c, piece)], preferred_element_type=F32
                )
                acc = acc + term.astype(BF16).astype(F32)
            new = (res_ref[rows, pl.ds(c, piece)].astype(F32) + acc).astype(BF16)
            mid[rows, pl.ds(c, piece)] = new
            wide = new.astype(F32)
            squares = squares + jnp.sum(wide * wide, axis=-1, keepdims=True)
        scale = lax.rsqrt(squares * (1.0 / width) + EPS)
        for c in range(0, width, piece):
            wide = mid[rows, pl.ds(c, piece)].astype(F32)
            normed[rows, pl.ds(c, piece)] = (
                wide * scale * gain_ref[:, pl.ds(c, piece)]
            ).astype(BF16)
        return carry

    lax.fori_loop(0, 4, mix, 0)

    for kind in range(2):
        own_local[kind].wait()

    def take_up(c, carry):
        there, valid, above = candidate(c)

        @pl.when(valid)
        def _():
            for kind in range(2):
                up_copy(kind, there * PAIR + (1 - side), 2).wait_recv()

        return carry

    lax.fori_loop(0, 2 * line - 1, take_up, 0)

    def project(i, carry):
        base = pl.multiple_of(i * tile, tile)
        left = normed[pl.ds(base, tile), :]
        rows = pl.ds(pl.multiple_of(base + EDGE, EDGE), tile)
        for weight, dest in ((wg, upg), (wv, upv)):
            for c in range(0, hid, piece):
                term = jnp.dot(left, weight[:, pl.ds(c, piece)], preferred_element_type=F32)
                dest[rows, pl.ds(c, piece)] = term.astype(BF16).astype(F32)
        return carry

    lax.fori_loop(0, 4, project, 0)

    def edge_low(kind):
        ref = (upg, upv)[kind]
        return remote(
            ref.at[pl.ds(EDGE, EDGE), :],
            ref.at[pl.ds(EDGE + tok, EDGE), :],
            edge_send.at[0, kind],
            edge_recv.at[1, kind],
            sp=me - 1,
        )

    def edge_high(kind):
        ref = (upg, upv)[kind]
        return remote(
            ref.at[pl.ds(tok, EDGE), :],
            ref.at[pl.ds(0, EDGE), :],
            edge_send.at[1, kind],
            edge_recv.at[0, kind],
            sp=me + 1,
        )

    none = jnp.zeros((EDGE, hid), F32)
    for kind in range(2):
        pl.when(has_low)(edge_low(kind).start)
        pl.when(has_high)(edge_high(kind).start)

    @pl.when(jnp.logical_not(has_low))
    def _():
        upg[pl.ds(0, EDGE), :] = none
        upv[pl.ds(0, EDGE), :] = none

    @pl.when(jnp.logical_not(has_high))
    def _():
        upg[pl.ds(EDGE + tok, EDGE), :] = none
        upv[pl.ds(EDGE + tok, EDGE), :] = none

    for kind in range(2):
        pl.when(has_low)(edge_high(kind).wait_recv)
        pl.when(has_high)(edge_low(kind).wait_recv)

    def gate(i, carry):
        base = pl.multiple_of(i * WINDOW, WINDOW)
        for c in range(0, hid, 256):
            lanes = pl.ds(c, 256)

            def convolve(ref, taps):
                field = ref[pl.ds(base, WINDOW + 2 * EDGE), lanes]
                return (
                    field[EDGE - 1 : EDGE - 1 + WINDOW] * taps[0:1, lanes]
                    + field[EDGE : EDGE + WINDOW] * taps[1:2, lanes]
                    + field[EDGE + 1 : EDGE + 1 + WINDOW] * taps[2:3, lanes]
                )

            g = convolve(upg, tg_ref)
            v = convolve(upv, tv_ref)
            hidden[pl.ds(base, WINDOW), lanes] = (g / (1.0 + jnp.exp(-g)) * v).astype(BF16)
        return carry

    lax.fori_loop(0, tok // WINDOW, gate, 0)

    def rs_copy(block, k):
        return remote(
            terms.at[block, pl.ds(pl.multiple_of(peers[k] * share, share), share), :],
            rbuf.at[my_tp, block],
            rs_send.at[block, k],
            rs_recv.at[block, my_tp],
            tp=peers[k],
        )

    def process(block):
        def part(i, carry):
            rows = pl.ds(pl.multiple_of(i * tile, tile), tile)
            terms[block, rows, :] = jnp.dot(
                hidden[rows, :], wd[block], preferred_element_type=F32
            ).astype(BF16)
            return carry

        lax.fori_loop(0, 4, part, 0)
        for k in range(tp - 1):
            rs_copy(block, k).start()

    own_local[2].wait()

    def down(c, carry):
        there, valid, above = candidate(c)
        block = there * PAIR + side

        @pl.when(valid)
        def _():
            @pl.when(c > 0)
            def _():
                dn_copy(block, 2).wait_recv()
                dn_copy(block, 2).start()
                pl.when(above & can_down)(dn_copy(block, 0).start)
                pl.when(jnp.logical_not(above) & can_up)(dn_copy(block, 1).start)

            process(block)

        before, was_valid, _ = candidate(jnp.maximum(c - 1, 0))

        @pl.when(was_valid & (c > 0))
        def _():
            other = before * PAIR + (1 - side)
            dn_copy(other, 2).wait_recv()
            process(other)

        return carry

    lax.fori_loop(0, 2 * line, down, 0)

    my_rows = pl.ds(pl.multiple_of(my_tp * share, share), share)

    for block in range(sp):
        lanes = pl.ds(block * cols, cols)
        acc = mid[my_rows, lanes].astype(F32) + terms[block, my_rows, :].astype(F32)
        for k in range(tp - 1):
            src = peers[k]
            remote(
                rbuf.at[src, block],
                rbuf.at[src, block],
                rs_send.at[block, k],
                rs_recv.at[block, src],
                tp=src,
            ).wait_recv()
            acc = acc + rbuf[src, block].astype(F32)
        out_ref[:, lanes] = acc.astype(BF16)

    def drain(c, carry):
        there, valid, above = candidate(c)
        block = there * PAIR + side
        goes_down = can_down & (above | (c == 0))
        goes_up = can_up & (jnp.logical_not(above) | (c == 0))

        @pl.when(valid)
        def _():
            for copy in (
                lambda way: up_copy(0, block, way),
                lambda way: up_copy(1, block, way),
                lambda way: dn_copy(block, way),
            ):
                copy(2).wait_send()
                pl.when(goes_down)(copy(0).wait_send)
                pl.when(goes_up)(copy(1).wait_send)

        return carry

    lax.fori_loop(0, 2 * line - 1, drain, 0)
    for k in range(tp - 1):
        wo_copy(k).wait_send()
        att_copy(k).wait_send()
    pl.when(has_low)(kv_low.wait_send)
    pl.when(has_high)(kv_high.wait_send)
    for kind in range(2):
        pl.when(has_low)(edge_low(kind).wait_send)
        pl.when(has_high)(edge_high(kind).wait_send)

    def drain_rs(block, carry):
        for k in range(tp - 1):
            rs_copy(block, k).wait_send()
        return carry

    lax.fori_loop(0, sp, drain_rs, 0)


def kernel_shards(
    sp,
    tp,
    residual,
    query,
    key,
    value,
    sink,
    norm_gain,
    w_out,
    w_gate,
    w_value,
    conv_gate,
    conv_value,
    w_down,
):
    tok, width = residual.shape
    depth, hid = w_gate.shape
    cols = w_down.shape[1]
    heads = query.shape[1] // HD
    offset = lax.axis_index("sp") * tok
    positions = (offset + jnp.arange(tok, dtype=jnp.int32)).astype(F32)
    turned_query = rotate(query, positions) * jnp.asarray(HD**-0.5, BF16)
    turned_key = rotate(key, positions)
    band = jnp.concatenate([turned_key, value], axis=1)
    by_head = turned_query.reshape(tok, heads, HD).transpose(1, 0, 2)
    by_head = jnp.pad(by_head, ((0, 0), (0, 0), (0, HD)))
    vmem = pl.BlockSpec(memory_space=pltpu.VMEM)
    smem = pl.BlockSpec(memory_space=pltpu.SMEM)
    dma = pltpu.SemaphoreType.DMA
    return pl.pallas_call(
        functools.partial(layer_kernel, sp, tp),
        out_shape=jax.ShapeDtypeStruct((tok // tp, width), BF16),
        in_specs=[vmem, vmem, smem] + [vmem] * 8,
        out_specs=vmem,
        scratch_shapes=[
            pltpu.VMEM((tok + 2 * WINDOW, 2 * HD), BF16),
            pltpu.VMEM((tp, tok, heads * HD), BF16),
            pltpu.VMEM((tp,) + w_out.shape, BF16),
            pltpu.VMEM((sp * depth, hid), BF16),
            pltpu.VMEM((sp * depth, hid), BF16),
            pltpu.VMEM((sp, hid, cols), BF16),
            pltpu.VMEM((tok, width), BF16),
            pltpu.VMEM((tok, width), BF16),
            pltpu.VMEM((tok + 2 * EDGE, hid), F32),
            pltpu.VMEM((tok + 2 * EDGE, hid), F32),
            pltpu.VMEM((tok, hid), BF16),
            pltpu.VMEM((sp, tok, cols), BF16),
            pltpu.VMEM((tp, sp, tok // tp, cols), BF16),
            dma((5,)),
            dma((2, sp, 3)),
            dma((2, sp)),
            dma((sp, 3)),
            dma((sp,)),
            dma((tp - 1,)),
            dma((tp,)),
            dma((tp - 1,)),
            dma((tp,)),
            dma((2,)),
            dma((2,)),
            dma((2, 2)),
            dma((2, 2)),
            dma((sp, tp - 1)),
            dma((sp, tp)),
        ],
        compiler_params=pltpu.CompilerParams(
            collective_id=0, has_side_effects=True, vmem_limit_bytes=66 * 1000 * 1000
        ),
        name="layer",
    )(
        by_head,
        band,
        sink,
        residual,
        norm_gain.reshape(1, -1),
        w_out,
        w_gate,
        w_value,
        conv_gate.astype(F32),
        conv_value.astype(F32),
        w_down,
    )


def solution(mesh):
    sp, tp = mesh.shape["sp"], mesh.shape["tp"]

    def shards(*args):
        if args[11].shape[1] % 128 or sp % PAIR:
            return plain_shards(*args)
        return kernel_shards(sp, tp, *args)

    return jax.shard_map(
        shards,
        mesh=mesh,
        in_specs=(
            P("sp", None),
            P("sp", "tp"),
            P("sp", "tp"),
            P("sp", "tp"),
            P("tp"),
            P(),
            P("tp", None),
            P("sp", "tp"),
            P("sp", "tp"),
            P(None, "tp"),
            P(None, "tp"),
            P("tp", "sp"),
        ),
        out_specs=P(("sp", "tp"), None),
        check_vma=False,
    )
```

```python
import functools

import jax
import jax.numpy as jnp
import numpy as np
from jax import lax
from jax.experimental import pallas as pl
from jax.experimental.pallas import tpu as pltpu
from jax.sharding import PartitionSpec as P

HD = 64
WINDOW = 128


THETA = 10000.0
EPS = 1e-06


def extended(block, sides, width):
    for axis, dim in sides:
        count = lax.axis_size(axis)
        forward = [(i, i + 1) for i in range(count - 1)]
        backward = [(target, source) for source, target in forward]
        low = lax.ppermute(
            lax.slice_in_dim(block, block.shape[dim] - width, None, axis=dim), axis, forward
        )
        high = lax.ppermute(lax.slice_in_dim(block, 0, width, axis=dim), axis, backward)
        block = jnp.concatenate([low, block, high], axis=dim)
    return block


def rotate(field, positions):
    count = field.shape[0]
    parts = field.astype(jnp.float32).reshape(count, -1, HD)
    inverse = 1.0 / THETA ** (jnp.arange(0, HD, 2, dtype=jnp.float32) / HD)
    angle = positions[:, None] * inverse[None, :]
    cosine = jnp.cos(angle)[:, None, :]
    sine = jnp.sin(angle)[:, None, :]
    first = parts[..., : HD // 2]
    second = parts[..., HD // 2 :]
    turned = jnp.concatenate(
        [first * cosine - second * sine, second * cosine + first * sine], axis=-1
    )
    return turned.reshape(count, -1).astype(jnp.bfloat16)


def band_attention(queries, keys, values, sinks, start, total):
    count = queries.shape[0]
    blocks = count // WINDOW
    kv_local = keys.shape[1] // HD
    group = queries.shape[1] // (kv_local * HD)
    query_blocks = queries.reshape(blocks, WINDOW, kv_local, group, HD)
    key_band = jnp.concatenate(
        [
            keys[i * WINDOW : i * WINDOW + count].reshape(blocks, WINDOW, kv_local, HD)
            for i in range(3)
        ],
        axis=1,
    )
    value_band = jnp.concatenate(
        [
            values[i * WINDOW : i * WINDOW + count].reshape(blocks, WINDOW, kv_local, HD)
            for i in range(3)
        ],
        axis=1,
    )
    scores = jnp.einsum(
        "nqkgd,njkd->nkgqj", query_blocks, key_band, preferred_element_type=jnp.float32
    ) * HD ** (-0.5)
    block_ids = jnp.arange(blocks, dtype=jnp.int32)[:, None]
    query_pos = start + block_ids * WINDOW + jnp.arange(WINDOW, dtype=jnp.int32)[None, :]
    key_pos = start - WINDOW + block_ids * WINDOW + jnp.arange(3 * WINDOW, dtype=jnp.int32)[None, :]
    valid = (
        (key_pos[:, None, :] >= 0)
        & (key_pos[:, None, :] < total)
        & (jnp.abs(query_pos[:, :, None] - key_pos[:, None, :]) <= WINDOW)
    )
    scores = jnp.where(valid[:, None, None], scores, -1e30)
    sink_col = sinks.reshape(1, kv_local, group, 1, 1)
    top = jnp.maximum(jnp.max(scores, axis=-1, keepdims=True), sink_col)
    weights = jnp.exp(scores - top)
    denom = jnp.sum(weights, axis=-1, keepdims=True) + jnp.exp(sink_col - top)
    probs = (weights / denom).astype(jnp.bfloat16)
    out = jnp.einsum("nkgqj,njkd->nqkgd", probs, value_band, preferred_element_type=jnp.float32)
    return out.reshape(count, kv_local * group * HD).astype(jnp.bfloat16)


def rmsnorm(field, gain):
    wide = field.astype(jnp.float32)
    scale = lax.rsqrt(jnp.mean(wide * wide, axis=-1, keepdims=True) + EPS)
    return (wide * scale * gain).astype(jnp.bfloat16)


def plain_shards(
    residual,
    query,
    key,
    value,
    sink,
    norm_gain,
    w_out,
    w_gate,
    w_value,
    conv_gate,
    conv_value,
    w_down,
):
    tok_rows = query.shape[0]
    offset = lax.axis_index("sp") * tok_rows
    total = tok_rows * lax.axis_size("sp")
    share = tok_rows // lax.axis_size("tp")
    tp_index = lax.axis_index("tp")
    positions = (offset + jnp.arange(tok_rows, dtype=jnp.int32)).astype(jnp.float32)
    turned_query = rotate(query, positions)
    turned_key = rotate(key, positions)
    key_width = key.shape[1]
    band = jnp.concatenate([turned_key, value], axis=1)
    edged = extended(band, (("sp", 0),), WINDOW)
    attended = band_attention(
        turned_query, edged[:, :key_width], edged[:, key_width:], sink, offset, total
    )
    partial_value = jnp.dot(attended, w_out, preferred_element_type=jnp.float32)
    mix_full = lax.psum(partial_value.astype(jnp.bfloat16), "tp").astype(jnp.float32)
    mid_full = (residual.astype(jnp.float32) + mix_full).astype(jnp.bfloat16)
    normed = rmsnorm(mid_full, norm_gain)
    mid_rows = lax.dynamic_slice_in_dim(mid_full, tp_index * share, share, 0)
    gate_full, value_full = (
        lax.all_gather(w_gate, "sp", axis=0, tiled=True),
        lax.all_gather(w_value, "sp", axis=0, tiled=True),
    )
    gate_up = jnp.dot(normed, gate_full, preferred_element_type=jnp.float32).astype(jnp.bfloat16)
    value_up = jnp.dot(normed, value_full, preferred_element_type=jnp.float32).astype(jnp.bfloat16)
    hidden_width = gate_up.shape[1]
    stacked = jnp.concatenate([gate_up, value_up], axis=1)
    edged_up = extended(stacked, (("sp", 0),), 1).astype(jnp.float32)
    taps = jnp.concatenate([conv_gate, conv_value], axis=1).astype(jnp.float32)
    convolved = edged_up[:-2] * taps[0] + edged_up[1:-1] * taps[1] + edged_up[2:] * taps[2]
    hidden = (jax.nn.silu(convolved[:, :hidden_width]) * convolved[:, hidden_width:]).astype(
        jnp.bfloat16
    )
    terms = jnp.dot(
        hidden, lax.all_gather(w_down, "sp", axis=1, tiled=True), preferred_element_type=jnp.float32
    )
    ffn_rows = lax.psum_scatter(
        terms.astype(jnp.bfloat16), "tp", scatter_dimension=0, tiled=True
    ).astype(jnp.float32)
    return (mid_rows.astype(jnp.float32) + ffn_rows).astype(jnp.bfloat16)


F32 = jnp.float32
BF16 = jnp.bfloat16
PAIR = 2
EDGE = 8


def layer_kernel(
    sp,
    tp,
    q_ref,
    band_ref,
    cos_ref,
    sin_ref,
    base_ref,
    sink_ref,
    res_ref,
    gain_ref,
    wo_ref,
    wg_ref,
    wv_ref,
    tg_ref,
    tv_ref,
    wd_ref,
    out_ref,
    band,
    key_value,
    value_key,
    att,
    wo,
    wg,
    wv,
    wd,
    mid,
    normed,
    upg,
    upv,
    hidden,
    terms,
    near,
    pair_sum,
    far,
    local_sem,
    up_send,
    up_recv,
    dn_send,
    dn_recv,
    wo_send,
    wo_recv,
    att_send,
    att_recv,
    kv_send,
    kv_recv,
    edge_send,
    edge_recv,
    near_send,
    near_recv,
    far_send,
    far_recv,
):
    me = lax.axis_index("sp")
    my_tp = lax.axis_index("tp")
    tok, width = mid.shape
    share = tok // tp
    line = sp // PAIR
    place = me // PAIR
    side = me % PAIR
    mate = place * PAIR + (1 - side)
    depth = wg_ref.shape[0]
    cols = wd_ref.shape[1]
    hid = wg_ref.shape[1]
    has_low = me > 0
    has_high = me < sp - 1
    can_down = place > 0
    can_up = place < line - 1
    buddy = my_tp + 1 - 2 * (my_tp % 2)
    across = lax.rem(my_tp + 2, tp)
    corner = lax.rem(buddy + 2, tp)
    peers = [buddy, across, corner]

    def remote(src, dst, send, recv, **where):
        return pltpu.make_async_remote_copy(
            src_ref=src,
            dst_ref=dst,
            send_sem=send,
            recv_sem=recv,
            device_id=where,
            device_id_type=pl.DeviceIdType.MESH,
        )

    barrier = pltpu.get_barrier_semaphore()

    def greet(**where):
        pl.semaphore_signal(
            barrier, inc=1, device_id=where, device_id_type=pl.DeviceIdType.MESH
        )

    greet(sp=mate)
    for peer in peers:
        greet(tp=peer)
    far_low = has_low & (side == 0)
    far_high = has_high & (side == PAIR - 1)
    pl.when(far_low)(lambda: greet(sp=me - 1))
    pl.when(far_high)(lambda: greet(sp=me + 1))
    pl.when(can_down)(lambda: greet(sp=me - PAIR))
    pl.when(can_up)(lambda: greet(sp=me + PAIR))
    count = tp
    for able in (far_low, far_high, can_down, can_up):
        count = count + jnp.where(able, 1, 0)
    pl.semaphore_wait(barrier, count)

    def up_slot(kind, block):
        return (wg, wv)[kind].at[pl.ds(pl.multiple_of(block * depth, depth), depth), :]

    def up_copy(kind, block, way, own=False):
        target = (me - PAIR, me + PAIR, mate)[way]
        slot = up_slot(kind, block)
        return remote(
            (wg_ref, wv_ref)[kind] if own else slot,
            slot,
            up_send.at[kind, block, way],
            up_recv.at[kind, block],
            sp=target,
        )

    def dn_copy(block, way, own=False):
        target = (me - PAIR, me + PAIR, mate)[way]
        slot = wd.at[block]
        return remote(
            wd_ref if own else slot, slot, dn_send.at[block, way], dn_recv.at[block], sp=target
        )

    def candidate(c):
        distance = (c + 1) // 2
        there = jnp.where(c % 2 == 1, place + distance, place - distance)
        valid = (there >= 0) & (there < line)
        above = there > place
        return there, valid, above

    def distance_of(there):
        return jnp.where(there > place, there - place, place - there)

    own_local = [
        pltpu.make_async_copy(wg_ref, up_slot(0, me), local_sem.at[0]),
        pltpu.make_async_copy(wv_ref, up_slot(1, me), local_sem.at[1]),
        pltpu.make_async_copy(wd_ref, wd.at[me], local_sem.at[2]),
        pltpu.make_async_copy(wo_ref, wo.at[my_tp], local_sem.at[3]),
        pltpu.make_async_copy(band_ref, band.at[pl.ds(WINDOW, tok), :], local_sem.at[4]),
        pltpu.make_async_copy(res_ref, mid, local_sem.at[5]),
    ]

    kv_low = remote(
        band_ref.at[pl.ds(0, WINDOW), :],
        band.at[pl.ds(WINDOW + tok, WINDOW), :],
        kv_send.at[0],
        kv_recv.at[1],
        sp=me - 1,
    )
    kv_high = remote(
        band_ref.at[pl.ds(tok - WINDOW, WINDOW), :],
        band.at[pl.ds(0, WINDOW), :],
        kv_send.at[1],
        kv_recv.at[0],
        sp=me + 1,
    )
    pl.when(has_low)(kv_low.start)
    pl.when(has_high)(kv_high.start)
    for copy in own_local:
        copy.start()
    for kind in range(2):
        up_copy(kind, me, 2, True).start()
        pl.when(can_down)(up_copy(kind, me, 0, True).start)
        pl.when(can_up)(up_copy(kind, me, 1, True).start)

    def wo_copy(k, own=True):
        slot = wo.at[my_tp if own else across]
        return remote(
            wo_ref if own else slot,
            slot,
            wo_send.at[k],
            wo_recv.at[my_tp if own else across],
            tp=(buddy, across, buddy)[k],
        )

    def att_copy(k):
        slot = att.at[across if k == 2 else my_tp]
        return remote(
            slot,
            slot,
            att_send.at[k],
            att_recv.at[across if k == 2 else my_tp],
            tp=(buddy, across, buddy)[k],
        )

    def arrived(ref, recv, source):
        slot = ref.at[source]
        return remote(slot, slot, wo_send.at[0], recv.at[source], tp=buddy)

    wo_copy(1).start()
    wo_copy(0).start()

    blank = jnp.zeros((WINDOW, band.shape[1]), BF16)

    @pl.when(jnp.logical_not(has_low))
    def _():
        band[pl.ds(0, WINDOW), :] = blank

    @pl.when(jnp.logical_not(has_high))
    def _():
        band[pl.ds(WINDOW + tok, WINDOW), :] = blank

    own_local[4].wait()
    pl.when(has_low)(kv_high.wait_recv)
    pl.when(has_high)(kv_low.wait_recv)
    heads = q_ref.shape[1] // HD
    span = 3 * WINDOW
    total = tok * sp
    lane = lax.broadcasted_iota(jnp.int32, (WINDOW, 2 * HD), 1)
    early = lane % HD < HD // 2
    low = lane < HD

    def turn(field, start):
        rows = pl.ds(start, WINDOW)
        base_cos = base_ref[0:1, :]
        base_sin = base_ref[1:2, :]
        cosine = base_cos * cos_ref[rows, :] - base_sin * sin_ref[rows, :]
        sine = base_sin * cos_ref[rows, :] + base_cos * sin_ref[rows, :]
        ahead = pltpu.roll(field, 2 * HD - HD // 2, 1)
        behind = pltpu.roll(field, HD // 2, 1)
        return field * cosine + jnp.where(early, -ahead, behind) * sine

    def turn_keys(i, carry):
        start = pl.multiple_of(i * WINDOW, WINDOW)
        field = band[pl.ds(start, WINDOW), :].astype(F32)
        field = jnp.where(low, turn(field, start), field)
        key_value[pl.ds(start, WINDOW), :] = field.astype(BF16)
        value_key[pl.ds(start, WINDOW), :] = pltpu.roll(field, HD, 1).astype(BF16)
        return carry

    lax.fori_loop(0, tok // WINDOW + 2, turn_keys, 0)

    def attend(i, carry):
        start = pl.multiple_of(i * WINDOW, WINDOW)
        straight = key_value[pl.ds(start, span), :]
        crossed = value_key[pl.ds(start, span), :]
        row = lax.broadcasted_iota(jnp.int32, (WINDOW, span), 0)
        col = lax.broadcasted_iota(jnp.int32, (WINDOW, span), 1)
        key_pos = col + (me * tok - WINDOW + start)
        valid = (col >= row) & (col <= row + 2 * WINDOW) & (key_pos >= 0) & (key_pos < total)

        def head(query, sink, keys, values):
            scores = lax.dot_general(
                query, keys, (((1,), (1,)), ((), ())), preferred_element_type=F32
            )
            scores = jnp.where(valid, scores, -1e30)
            top = jnp.maximum(jnp.max(scores, axis=-1, keepdims=True), sink)
            weights = jnp.exp(scores - top)
            denom = jnp.sum(weights, axis=-1, keepdims=True) + jnp.exp(sink - top)
            probs = (weights * (1.0 / denom)).astype(BF16)
            return jnp.dot(probs, values, preferred_element_type=F32)

        for h in range(0, heads, 2):
            lanes = pl.ds(h * HD, 2 * HD)
            field = q_ref[pl.ds(start, WINDOW), lanes].astype(F32)
            field = turn(field, pl.multiple_of(start + WINDOW, WINDOW)) * HD**-0.5
            even = head(
                jnp.where(low, field, 0.0).astype(BF16), sink_ref[h], straight, crossed
            )
            odd = head(
                jnp.where(low, 0.0, field).astype(BF16), sink_ref[h + 1], crossed, straight
            )
            att[my_tp, pl.ds(start, WINDOW), lanes] = jnp.where(low, even, odd).astype(BF16)
        return carry

    lax.fori_loop(0, tok // WINDOW, attend, 0)
    att_copy(1).start()
    att_copy(0).start()

    def pass_up(c, carry):
        there, valid, above = candidate(c)
        block = there * PAIR + side

        @pl.when(valid)
        def _():
            for kind in range(2):
                up_copy(kind, block, 2).wait_recv()
                direct = (kind == 1) | (distance_of(there) > 1)
                pl.when(direct)(up_copy(kind, block, 2).start)
                pl.when(above & can_down)(up_copy(kind, block, 0).start)
                pl.when(jnp.logical_not(above) & can_up)(up_copy(kind, block, 1).start)

        return carry

    def start_down():
        dn_copy(me, 2, True).start()
        pl.when(can_down)(dn_copy(me, 0, True).start)
        pl.when(can_up)(dn_copy(me, 1, True).start)

    def pass_down(c, carry):
        there, valid, above = candidate(c)
        block = there * PAIR + side

        @pl.when(valid)
        def _():
            dn_copy(block, 2).wait_recv()
            dn_copy(block, 2).start()
            pl.when(above & can_down)(dn_copy(block, 0).start)
            pl.when(jnp.logical_not(above) & can_up)(dn_copy(block, 1).start)

        return carry

    up_copy(0, mate, 2).wait_recv()
    pl.when(can_down)(up_copy(0, mate, 0).start)
    pl.when(can_up)(up_copy(0, mate, 1).start)
    lax.fori_loop(1, 3, pass_up, 0)
    arrived(wo, wo_recv, across).wait_recv()
    wo_copy(2, False).start()
    arrived(att, att_recv, across).wait_recv()
    att_copy(2).start()
    lax.fori_loop(3, 2 * line - 1, pass_up, 0)
    start_down()

    own_local[3].wait()
    own_local[5].wait()
    for source in (buddy, corner):
        arrived(wo, wo_recv, source).wait_recv()
        arrived(att, att_recv, source).wait_recv()
    tile = tok // 4
    piece = 512

    def mix(i, carry):
        rows = pl.ds(pl.multiple_of(i * tile, tile), tile)
        squares = jnp.zeros((tile, 1), F32)
        for c in range(0, width, piece):
            acc = jnp.zeros((tile, piece), F32)
            for k in range(tp):
                term = jnp.dot(
                    att[k, rows, :], wo[k, :, pl.ds(c, piece)], preferred_element_type=F32
                )
                acc = acc + term.astype(BF16).astype(F32)
            new = (mid[rows, pl.ds(c, piece)].astype(F32) + acc).astype(BF16)
            mid[rows, pl.ds(c, piece)] = new
            wide = new.astype(F32)
            squares = squares + jnp.sum(wide * wide, axis=-1, keepdims=True)
        scale = lax.rsqrt(squares * (1.0 / width) + EPS)
        for c in range(0, width, piece):
            wide = mid[rows, pl.ds(c, piece)].astype(F32)
            normed[rows, pl.ds(c, piece)] = (
                wide * scale * gain_ref[:, pl.ds(c, piece)]
            ).astype(BF16)
        return carry

    lax.fori_loop(0, 4, mix, 0)

    for kind in range(2):
        own_local[kind].wait()

    def take_up(c, carry):
        there, valid, above = candidate(c)

        @pl.when(valid)
        def _():
            other = there * PAIR + (1 - side)
            pl.when(c > 0)(up_copy(0, other, 2).wait_recv)
            up_copy(1, other, 2).wait_recv()

        return carry

    lax.fori_loop(0, 2 * line - 1, take_up, 0)

    def project(i, carry):
        base = pl.multiple_of(i * tile, tile)
        left = normed[pl.ds(base, tile), :]
        rows = pl.ds(pl.multiple_of(base + EDGE, EDGE), tile)
        for weight, dest in ((wg, upg), (wv, upv)):
            for c in range(0, hid, piece):
                term = jnp.dot(left, weight[:, pl.ds(c, piece)], preferred_element_type=F32)
                dest[rows, pl.ds(c, piece)] = term.astype(BF16).astype(F32)
        return carry

    lax.fori_loop(0, 4, project, 0)

    def edge_low(kind):
        ref = (upg, upv)[kind]
        return remote(
            ref.at[pl.ds(EDGE, EDGE), :],
            ref.at[pl.ds(EDGE + tok, EDGE), :],
            edge_send.at[0, kind],
            edge_recv.at[1, kind],
            sp=me - 1,
        )

    def edge_high(kind):
        ref = (upg, upv)[kind]
        return remote(
            ref.at[pl.ds(tok, EDGE), :],
            ref.at[pl.ds(0, EDGE), :],
            edge_send.at[1, kind],
            edge_recv.at[0, kind],
            sp=me + 1,
        )

    none = jnp.zeros((EDGE, hid), F32)
    lax.fori_loop(1, 3, pass_down, 0)
    for kind in range(2):
        pl.when(has_low)(edge_low(kind).start)
        pl.when(has_high)(edge_high(kind).start)

    @pl.when(jnp.logical_not(has_low))
    def _():
        upg[pl.ds(0, EDGE), :] = none
        upv[pl.ds(0, EDGE), :] = none

    @pl.when(jnp.logical_not(has_high))
    def _():
        upg[pl.ds(EDGE + tok, EDGE), :] = none
        upv[pl.ds(EDGE + tok, EDGE), :] = none

    for kind in range(2):
        pl.when(has_low)(edge_high(kind).wait_recv)
        pl.when(has_high)(edge_low(kind).wait_recv)

    def gate(i, carry):
        base = pl.multiple_of(i * WINDOW, WINDOW)
        for c in range(0, hid, 256):
            lanes = pl.ds(c, 256)

            def convolve(ref, taps):
                field = ref[pl.ds(base, WINDOW + 2 * EDGE), lanes]
                taps = taps[:, lanes].astype(F32)
                return (
                    field[EDGE - 1 : EDGE - 1 + WINDOW] * taps[0:1]
                    + field[EDGE : EDGE + WINDOW] * taps[1:2]
                    + field[EDGE + 1 : EDGE + 1 + WINDOW] * taps[2:3]
                )

            g = convolve(upg, tg_ref)
            v = convolve(upv, tv_ref)
            hidden[pl.ds(base, WINDOW), lanes] = (g / (1.0 + jnp.exp(-g)) * v).astype(BF16)
        return carry

    lax.fori_loop(0, tok // WINDOW, gate, 0)

    def rows_of(owner):
        return pl.ds(pl.multiple_of(owner * share, share), share)

    def near_copy(block, k):
        return remote(
            terms.at[block, rows_of((buddy, corner)[k]), :],
            near.at[k, block],
            near_send.at[block, k],
            near_recv.at[block, k],
            tp=buddy,
        )

    def far_copy(block):
        return remote(
            pair_sum.at[block], far.at[block], far_send.at[block], far_recv.at[block], tp=across
        )

    def pass_pair(block):
        near_copy(block, 1).wait_recv()
        both = terms[block, rows_of(across), :].astype(F32) + near[1, block].astype(F32)
        pair_sum[block] = both.astype(BF16)
        far_copy(block).start()

    def process(block):
        def part(i, carry):
            rows = pl.ds(pl.multiple_of(i * tile, tile), tile)
            terms[block, rows, :] = jnp.dot(
                hidden[rows, :], wd[block], preferred_element_type=F32
            ).astype(BF16)
            return carry

        lax.fori_loop(0, 4, part, 0)
        near_copy(block, 1).start()
        near_copy(block, 0).start()

    own_local[2].wait()

    def down(c, carry):
        there, valid, above = candidate(c)
        block = there * PAIR + side

        @pl.when(valid)
        def _():
            @pl.when(c > 2)
            def _():
                pass_down(c, 0)

            process(block)

        before, was_valid, _ = candidate(jnp.maximum(c - 1, 0))

        @pl.when(was_valid & (c > 0))
        def _():
            other = before * PAIR + (1 - side)
            dn_copy(other, 2).wait_recv()
            process(other)
            pass_pair(before * PAIR + side)

        earlier, was_valid, _ = candidate(jnp.maximum(c - 2, 0))

        @pl.when(was_valid & (c > 1))
        def _():
            pass_pair(earlier * PAIR + (1 - side))

        return carry

    lax.fori_loop(0, 2 * line + 1, down, 0)

    my_rows = pl.ds(pl.multiple_of(my_tp * share, share), share)

    for block in range(sp):
        lanes = pl.ds(block * cols, cols)
        acc = mid[my_rows, lanes].astype(F32) + terms[block, my_rows, :].astype(F32)
        near_copy(block, 0).wait_recv()
        far_copy(block).wait_recv()
        acc = acc + near[0, block].astype(F32) + far[block].astype(F32)
        out_ref[:, lanes] = acc.astype(BF16)

    def drain(c, carry):
        there, valid, above = candidate(c)
        block = there * PAIR + side
        goes_down = can_down & (above | (c == 0))
        goes_up = can_up & (jnp.logical_not(above) | (c == 0))

        @pl.when(valid)
        def _():
            direct = (distance_of(there) > 1) | (c == 0)
            for kind, copy in enumerate(
                (
                    lambda way: up_copy(0, block, way),
                    lambda way: up_copy(1, block, way),
                    lambda way: dn_copy(block, way),
                )
            ):
                pl.when(direct | (kind > 0))(copy(2).wait_send)
                pl.when(goes_down)(copy(0).wait_send)
                pl.when(goes_up)(copy(1).wait_send)

        return carry

    pl.when(can_down)(up_copy(0, mate, 0).wait_send)
    pl.when(can_up)(up_copy(0, mate, 1).wait_send)
    lax.fori_loop(0, 2 * line - 1, drain, 0)
    for k in range(tp - 1):
        wo_copy(k, k < 2).wait_send()
        att_copy(k).wait_send()
    pl.when(has_low)(kv_low.wait_send)
    pl.when(has_high)(kv_high.wait_send)
    for kind in range(2):
        pl.when(has_low)(edge_low(kind).wait_send)
        pl.when(has_high)(edge_high(kind).wait_send)

    def drain_rs(block, carry):
        near_copy(block, 0).wait_send()
        near_copy(block, 1).wait_send()
        far_copy(block).wait_send()
        return carry

    lax.fori_loop(0, sp, drain_rs, 0)


def kernel_shards(
    sp,
    tp,
    residual,
    query,
    key,
    value,
    sink,
    norm_gain,
    w_out,
    w_gate,
    w_value,
    conv_gate,
    conv_value,
    w_down,
):
    tok, width = residual.shape
    depth, hid = w_gate.shape
    cols = w_down.shape[1]
    heads = query.shape[1] // HD
    share = tok // tp
    offset = lax.axis_index("sp") * tok
    band = jnp.concatenate([key, value], axis=1)
    inverse = THETA ** (-(np.arange(2 * HD) % (HD // 2)) * 2.0 / HD)
    angle = (np.arange(tok + 2 * WINDOW) - WINDOW)[:, None] * inverse[None, :]
    first = offset.astype(F32) * jnp.asarray(inverse, F32)
    base = jnp.stack([jnp.cos(first), jnp.sin(first)])
    vmem = pl.BlockSpec(memory_space=pltpu.VMEM)
    smem = pl.BlockSpec(memory_space=pltpu.SMEM)
    anywhere = pl.BlockSpec(memory_space=pl.ANY)
    dma = pltpu.SemaphoreType.DMA
    return pl.pallas_call(
        functools.partial(layer_kernel, sp, tp),
        out_shape=jax.ShapeDtypeStruct((tok // tp, width), BF16),
        in_specs=[vmem] * 5 + [smem, anywhere, vmem] + [anywhere] * 3 + [vmem] * 2 + [anywhere],
        out_specs=vmem,
        scratch_shapes=[
            pltpu.VMEM((tok + 2 * WINDOW, 2 * HD), BF16),
            pltpu.VMEM((tok + 2 * WINDOW, 2 * HD), BF16),
            pltpu.VMEM((tok + 2 * WINDOW, 2 * HD), BF16),
            pltpu.VMEM((tp, tok, heads * HD), BF16),
            pltpu.VMEM((tp,) + w_out.shape, BF16),
            pltpu.VMEM((sp * depth, hid), BF16),
            pltpu.VMEM((sp * depth, hid), BF16),
            pltpu.VMEM((sp, hid, cols), BF16),
            pltpu.VMEM((tok, width), BF16),
            pltpu.VMEM((tok, width), BF16),
            pltpu.VMEM((tok + 2 * EDGE, hid), F32),
            pltpu.VMEM((tok + 2 * EDGE, hid), F32),
            pltpu.VMEM((tok, hid), BF16),
            pltpu.VMEM((sp, tok, cols), BF16),
            pltpu.VMEM((2, sp, share, cols), BF16),
            pltpu.VMEM((sp, share, cols), BF16),
            pltpu.VMEM((sp, share, cols), BF16),
            dma((6,)),
            dma((2, sp, 3)),
            dma((2, sp)),
            dma((sp, 3)),
            dma((sp,)),
            dma((tp - 1,)),
            dma((tp,)),
            dma((tp - 1,)),
            dma((tp,)),
            dma((2,)),
            dma((2,)),
            dma((2, 2)),
            dma((2, 2)),
            dma((sp, 2)),
            dma((sp, 2)),
            dma((sp,)),
            dma((sp,)),
        ],
        compiler_params=pltpu.CompilerParams(
            collective_id=0, has_side_effects=True, vmem_limit_bytes=66 * 1000 * 1000
        ),
        name="layer",
    )(
        query,
        band,
        jnp.asarray(np.cos(angle), F32),
        jnp.asarray(np.sin(angle), F32),
        base,
        sink,
        residual,
        norm_gain.reshape(1, -1),
        w_out,
        w_gate,
        w_value,
        conv_gate,
        conv_value,
        w_down,
    )


def solution(mesh):
    sp, tp = mesh.shape["sp"], mesh.shape["tp"]

    def shards(*args):
        if args[11].shape[1] % 128 or sp % PAIR or tp != 4 or args[2].shape[1] != HD:
            return plain_shards(*args)
        return kernel_shards(sp, tp, *args)

    return jax.shard_map(
        shards,
        mesh=mesh,
        in_specs=(
            P("sp", None),
            P("sp", "tp"),
            P("sp", "tp"),
            P("sp", "tp"),
            P("tp"),
            P(),
            P("tp", None),
            P("sp", "tp"),
            P("sp", "tp"),
            P(None, "tp"),
            P(None, "tp"),
            P("tp", "sp"),
        ),
        out_specs=P(("sp", "tp"), None),
        check_vma=False,
    )
```

```python
import functools

import jax
import jax.numpy as jnp
import numpy as np
from jax import lax
from jax.experimental import pallas as pl
from jax.experimental.pallas import tpu as pltpu
from jax.sharding import PartitionSpec as P

HD = 64
WINDOW = 128


THETA = 10000.0
EPS = 1e-06


def extended(block, sides, width):
    for axis, dim in sides:
        count = lax.axis_size(axis)
        forward = [(i, i + 1) for i in range(count - 1)]
        backward = [(target, source) for source, target in forward]
        low = lax.ppermute(
            lax.slice_in_dim(block, block.shape[dim] - width, None, axis=dim), axis, forward
        )
        high = lax.ppermute(lax.slice_in_dim(block, 0, width, axis=dim), axis, backward)
        block = jnp.concatenate([low, block, high], axis=dim)
    return block


def rotate(field, positions):
    count = field.shape[0]
    parts = field.astype(jnp.float32).reshape(count, -1, HD)
    inverse = 1.0 / THETA ** (jnp.arange(0, HD, 2, dtype=jnp.float32) / HD)
    angle = positions[:, None] * inverse[None, :]
    cosine = jnp.cos(angle)[:, None, :]
    sine = jnp.sin(angle)[:, None, :]
    first = parts[..., : HD // 2]
    second = parts[..., HD // 2 :]
    turned = jnp.concatenate(
        [first * cosine - second * sine, second * cosine + first * sine], axis=-1
    )
    return turned.reshape(count, -1).astype(jnp.bfloat16)


def band_attention(queries, keys, values, sinks, start, total):
    count = queries.shape[0]
    blocks = count // WINDOW
    kv_local = keys.shape[1] // HD
    group = queries.shape[1] // (kv_local * HD)
    query_blocks = queries.reshape(blocks, WINDOW, kv_local, group, HD)
    key_band = jnp.concatenate(
        [
            keys[i * WINDOW : i * WINDOW + count].reshape(blocks, WINDOW, kv_local, HD)
            for i in range(3)
        ],
        axis=1,
    )
    value_band = jnp.concatenate(
        [
            values[i * WINDOW : i * WINDOW + count].reshape(blocks, WINDOW, kv_local, HD)
            for i in range(3)
        ],
        axis=1,
    )
    scores = jnp.einsum(
        "nqkgd,njkd->nkgqj", query_blocks, key_band, preferred_element_type=jnp.float32
    ) * HD ** (-0.5)
    block_ids = jnp.arange(blocks, dtype=jnp.int32)[:, None]
    query_pos = start + block_ids * WINDOW + jnp.arange(WINDOW, dtype=jnp.int32)[None, :]
    key_pos = start - WINDOW + block_ids * WINDOW + jnp.arange(3 * WINDOW, dtype=jnp.int32)[None, :]
    valid = (
        (key_pos[:, None, :] >= 0)
        & (key_pos[:, None, :] < total)
        & (jnp.abs(query_pos[:, :, None] - key_pos[:, None, :]) <= WINDOW)
    )
    scores = jnp.where(valid[:, None, None], scores, -1e30)
    sink_col = sinks.reshape(1, kv_local, group, 1, 1)
    top = jnp.maximum(jnp.max(scores, axis=-1, keepdims=True), sink_col)
    weights = jnp.exp(scores - top)
    denom = jnp.sum(weights, axis=-1, keepdims=True) + jnp.exp(sink_col - top)
    probs = (weights / denom).astype(jnp.bfloat16)
    out = jnp.einsum("nkgqj,njkd->nqkgd", probs, value_band, preferred_element_type=jnp.float32)
    return out.reshape(count, kv_local * group * HD).astype(jnp.bfloat16)


def rmsnorm(field, gain):
    wide = field.astype(jnp.float32)
    scale = lax.rsqrt(jnp.mean(wide * wide, axis=-1, keepdims=True) + EPS)
    return (wide * scale * gain).astype(jnp.bfloat16)


def plain_shards(
    residual,
    query,
    key,
    value,
    sink,
    norm_gain,
    w_out,
    w_gate,
    w_value,
    conv_gate,
    conv_value,
    w_down,
):
    tok_rows = query.shape[0]
    offset = lax.axis_index("sp") * tok_rows
    total = tok_rows * lax.axis_size("sp")
    share = tok_rows // lax.axis_size("tp")
    tp_index = lax.axis_index("tp")
    positions = (offset + jnp.arange(tok_rows, dtype=jnp.int32)).astype(jnp.float32)
    turned_query = rotate(query, positions)
    turned_key = rotate(key, positions)
    key_width = key.shape[1]
    band = jnp.concatenate([turned_key, value], axis=1)
    edged = extended(band, (("sp", 0),), WINDOW)
    attended = band_attention(
        turned_query, edged[:, :key_width], edged[:, key_width:], sink, offset, total
    )
    partial_value = jnp.dot(attended, w_out, preferred_element_type=jnp.float32)
    mix_full = lax.psum(partial_value.astype(jnp.bfloat16), "tp").astype(jnp.float32)
    mid_full = (residual.astype(jnp.float32) + mix_full).astype(jnp.bfloat16)
    normed = rmsnorm(mid_full, norm_gain)
    mid_rows = lax.dynamic_slice_in_dim(mid_full, tp_index * share, share, 0)
    gate_full, value_full = (
        lax.all_gather(w_gate, "sp", axis=0, tiled=True),
        lax.all_gather(w_value, "sp", axis=0, tiled=True),
    )
    gate_up = jnp.dot(normed, gate_full, preferred_element_type=jnp.float32).astype(jnp.bfloat16)
    value_up = jnp.dot(normed, value_full, preferred_element_type=jnp.float32).astype(jnp.bfloat16)
    hidden_width = gate_up.shape[1]
    stacked = jnp.concatenate([gate_up, value_up], axis=1)
    edged_up = extended(stacked, (("sp", 0),), 1).astype(jnp.float32)
    taps = jnp.concatenate([conv_gate, conv_value], axis=1).astype(jnp.float32)
    convolved = edged_up[:-2] * taps[0] + edged_up[1:-1] * taps[1] + edged_up[2:] * taps[2]
    hidden = (jax.nn.silu(convolved[:, :hidden_width]) * convolved[:, hidden_width:]).astype(
        jnp.bfloat16
    )
    terms = jnp.dot(
        hidden, lax.all_gather(w_down, "sp", axis=1, tiled=True), preferred_element_type=jnp.float32
    )
    ffn_rows = lax.psum_scatter(
        terms.astype(jnp.bfloat16), "tp", scatter_dimension=0, tiled=True
    ).astype(jnp.float32)
    return (mid_rows.astype(jnp.float32) + ffn_rows).astype(jnp.bfloat16)


F32 = jnp.float32
BF16 = jnp.bfloat16
PAIR = 2
HALVES = 2
PIECES = 2 * HALVES
EDGE = 8


def layer_kernel(
    sp,
    tp,
    q_ref,
    band_ref,
    cos_ref,
    sin_ref,
    base_ref,
    sink_ref,
    res_ref,
    gain_ref,
    wo_ref,
    wg_ref,
    wv_ref,
    tg_ref,
    tv_ref,
    wd_ref,
    out_ref,
    band,
    key_value,
    value_key,
    att,
    wo,
    wg,
    wv,
    wd,
    mid,
    normed,
    upg,
    upv,
    hidden,
    terms,
    near,
    pair_sum,
    far,
    local_sem,
    up_send,
    up_recv,
    dn_send,
    dn_recv,
    wo_send,
    wo_recv,
    att_send,
    att_recv,
    kv_send,
    kv_recv,
    edge_send,
    edge_recv,
    near_send,
    near_recv,
    far_send,
    far_recv,
):
    me = lax.axis_index("sp")
    my_tp = lax.axis_index("tp")
    tok, width = mid.shape
    share = tok // tp
    line = sp // PAIR
    place = me // PAIR
    side = me % PAIR
    mate = place * PAIR + (1 - side)
    depth = wg_ref.shape[0]
    half = depth // HALVES
    cols = wd_ref.shape[1]
    hid = wg_ref.shape[1]
    has_low = me > 0
    has_high = me < sp - 1
    can_down = place > 0
    can_up = place < line - 1
    buddy = my_tp + 1 - 2 * (my_tp % 2)
    across = lax.rem(my_tp + 2, tp)
    corner = lax.rem(buddy + 2, tp)
    peers = [buddy, across, corner]

    def remote(src, dst, send, recv, **where):
        return pltpu.make_async_remote_copy(
            src_ref=src,
            dst_ref=dst,
            send_sem=send,
            recv_sem=recv,
            device_id=where,
            device_id_type=pl.DeviceIdType.MESH,
        )

    barrier = pltpu.get_barrier_semaphore()

    def greet(**where):
        pl.semaphore_signal(
            barrier, inc=1, device_id=where, device_id_type=pl.DeviceIdType.MESH
        )

    greet(sp=mate)
    for peer in peers:
        greet(tp=peer)
    far_low = has_low & (side == 0)
    far_high = has_high & (side == PAIR - 1)
    pl.when(far_low)(lambda: greet(sp=me - 1))
    pl.when(far_high)(lambda: greet(sp=me + 1))
    pl.when(can_down)(lambda: greet(sp=me - PAIR))
    pl.when(can_up)(lambda: greet(sp=me + PAIR))
    count = tp
    for able in (far_low, far_high, can_down, can_up):
        count = count + jnp.where(able, 1, 0)
    pl.semaphore_wait(barrier, count)

    def up_slot(kind, block):
        start = pl.multiple_of(block * depth + kind % HALVES * half, half)
        return (wg, wv)[kind // HALVES].at[pl.ds(start, half), :]

    def up_copy(kind, block, way, own=False):
        target = (me - PAIR, me + PAIR, mate)[way]
        slot = up_slot(kind, block)
        return remote(
            (wg_ref, wv_ref)[kind // HALVES].at[pl.ds(kind % HALVES * half, half), :]
            if own
            else slot,
            slot,
            up_send.at[kind, block, way],
            up_recv.at[kind, block],
            sp=target,
        )

    def dn_copy(block, way, own=False):
        target = (me - PAIR, me + PAIR, mate)[way]
        slot = wd.at[block]
        return remote(
            wd_ref if own else slot, slot, dn_send.at[block, way], dn_recv.at[block], sp=target
        )

    def candidate(c):
        distance = (c + 1) // 2
        there = jnp.where(c % 2 == 1, place + distance, place - distance)
        valid = (there >= 0) & (there < line)
        above = there > place
        return there, valid, above

    def distance_of(there):
        return jnp.where(there > place, there - place, place - there)

    def up_rows(ref):
        return ref.at[pl.ds(pl.multiple_of(me * depth, depth), depth), :]

    own_local = [
        pltpu.make_async_copy(wg_ref, up_rows(wg), local_sem.at[0]),
        pltpu.make_async_copy(wv_ref, up_rows(wv), local_sem.at[1]),
        pltpu.make_async_copy(wd_ref, wd.at[me], local_sem.at[2]),
        pltpu.make_async_copy(wo_ref, wo.at[my_tp], local_sem.at[3]),
        pltpu.make_async_copy(band_ref, band.at[pl.ds(WINDOW, tok), :], local_sem.at[4]),
        pltpu.make_async_copy(res_ref, mid, local_sem.at[5]),
    ]

    kv_low = remote(
        band_ref.at[pl.ds(0, WINDOW), :],
        band.at[pl.ds(WINDOW + tok, WINDOW), :],
        kv_send.at[0],
        kv_recv.at[1],
        sp=me - 1,
    )
    kv_high = remote(
        band_ref.at[pl.ds(tok - WINDOW, WINDOW), :],
        band.at[pl.ds(0, WINDOW), :],
        kv_send.at[1],
        kv_recv.at[0],
        sp=me + 1,
    )
    pl.when(has_low)(kv_low.start)
    pl.when(has_high)(kv_high.start)
    for copy in own_local:
        copy.start()
    for kind in range(PIECES):
        up_copy(kind, me, 2, True).start()
        pl.when(can_down)(up_copy(kind, me, 0, True).start)
        pl.when(can_up)(up_copy(kind, me, 1, True).start)
    dn_copy(me, 2, True).start()

    def wo_copy(k, own=True):
        slot = wo.at[my_tp if own else across]
        return remote(
            wo_ref if own else slot,
            slot,
            wo_send.at[k],
            wo_recv.at[my_tp if own else across],
            tp=(buddy, across, buddy)[k],
        )

    def att_copy(k):
        slot = att.at[across if k == 2 else my_tp]
        return remote(
            slot,
            slot,
            att_send.at[k],
            att_recv.at[across if k == 2 else my_tp],
            tp=(buddy, across, buddy)[k],
        )

    def arrived(ref, recv, source):
        slot = ref.at[source]
        return remote(slot, slot, wo_send.at[0], recv.at[source], tp=buddy)

    wo_copy(1).start()
    wo_copy(0).start()

    blank = jnp.zeros((WINDOW, band.shape[1]), BF16)

    @pl.when(jnp.logical_not(has_low))
    def _():
        band[pl.ds(0, WINDOW), :] = blank

    @pl.when(jnp.logical_not(has_high))
    def _():
        band[pl.ds(WINDOW + tok, WINDOW), :] = blank

    own_local[4].wait()
    pl.when(has_low)(kv_high.wait_recv)
    pl.when(has_high)(kv_low.wait_recv)
    heads = q_ref.shape[1] // HD
    span = 3 * WINDOW
    total = tok * sp
    lane = lax.broadcasted_iota(jnp.int32, (WINDOW, 2 * HD), 1)
    early = lane % HD < HD // 2
    low = lane < HD

    def turn(field, start):
        rows = pl.ds(start, WINDOW)
        base_cos = base_ref[0:1, :]
        base_sin = base_ref[1:2, :]
        cosine = base_cos * cos_ref[rows, :] - base_sin * sin_ref[rows, :]
        sine = base_sin * cos_ref[rows, :] + base_cos * sin_ref[rows, :]
        ahead = pltpu.roll(field, 2 * HD - HD // 2, 1)
        behind = pltpu.roll(field, HD // 2, 1)
        return field * cosine + jnp.where(early, -ahead, behind) * sine

    def turn_keys(i, carry):
        start = pl.multiple_of(i * WINDOW, WINDOW)
        field = band[pl.ds(start, WINDOW), :].astype(F32)
        field = jnp.where(low, turn(field, start), field)
        key_value[pl.ds(start, WINDOW), :] = field.astype(BF16)
        value_key[pl.ds(start, WINDOW), :] = pltpu.roll(field, HD, 1).astype(BF16)
        return carry

    lax.fori_loop(0, tok // WINDOW + 2, turn_keys, 0)

    def attend(i, carry):
        start = pl.multiple_of(i * WINDOW, WINDOW)
        straight = key_value[pl.ds(start, span), :]
        crossed = value_key[pl.ds(start, span), :]
        row = lax.broadcasted_iota(jnp.int32, (WINDOW, span), 0)
        col = lax.broadcasted_iota(jnp.int32, (WINDOW, span), 1)
        key_pos = col + (me * tok - WINDOW + start)
        valid = (col >= row) & (col <= row + 2 * WINDOW) & (key_pos >= 0) & (key_pos < total)

        def head(query, sink, keys, values):
            scores = lax.dot_general(
                query, keys, (((1,), (1,)), ((), ())), preferred_element_type=F32
            )
            scores = jnp.where(valid, scores, -1e30)
            top = jnp.maximum(jnp.max(scores, axis=-1, keepdims=True), sink)
            weights = jnp.exp(scores - top)
            denom = jnp.sum(weights, axis=-1, keepdims=True) + jnp.exp(sink - top)
            probs = (weights * (1.0 / denom)).astype(BF16)
            return jnp.dot(probs, values, preferred_element_type=F32)

        for h in range(0, heads, 2):
            lanes = pl.ds(h * HD, 2 * HD)
            field = q_ref[pl.ds(start, WINDOW), lanes].astype(F32)
            field = turn(field, pl.multiple_of(start + WINDOW, WINDOW)) * HD**-0.5
            even = head(
                jnp.where(low, field, 0.0).astype(BF16), sink_ref[h], straight, crossed
            )
            odd = head(
                jnp.where(low, 0.0, field).astype(BF16), sink_ref[h + 1], crossed, straight
            )
            att[my_tp, pl.ds(start, WINDOW), lanes] = jnp.where(low, even, odd).astype(BF16)
        return carry

    lax.fori_loop(0, tok // WINDOW, attend, 0)
    att_copy(1).start()
    att_copy(0).start()

    def pass_up(c, kind):
        there, valid, above = candidate(c)
        block = there * PAIR + side

        @pl.when(valid)
        def _():
            up_copy(kind, block, 2).wait_recv()
            if c > 2 or kind >= HALVES:
                up_copy(kind, block, 2).start()
            pl.when(above & can_down)(up_copy(kind, block, 0).start)
            pl.when(jnp.logical_not(above) & can_up)(up_copy(kind, block, 1).start)

    def start_down():
        pl.when(can_down)(dn_copy(me, 0, True).start)
        pl.when(can_up)(dn_copy(me, 1, True).start)

    def pass_down(c, carry):
        there, valid, above = candidate(c)
        block = there * PAIR + side

        @pl.when(valid)
        def _():
            dn_copy(block, 2).wait_recv()
            dn_copy(block, 2).start()
            pl.when(above & can_down)(dn_copy(block, 0).start)
            pl.when(jnp.logical_not(above) & can_up)(dn_copy(block, 1).start)

        return carry

    for kind in range(PIECES):
        for c in (1, 2):
            pass_up(c, kind)
    for kind in range(HALVES):
        up_copy(kind, mate, 2).wait_recv()
        pl.when(can_down)(up_copy(kind, mate, 0).start)
        pl.when(can_up)(up_copy(kind, mate, 1).start)
    arrived(wo, wo_recv, across).wait_recv()
    wo_copy(2, False).start()
    arrived(att, att_recv, across).wait_recv()
    att_copy(2).start()
    for kind in range(PIECES):
        for c in (3, 4):
            if c < 2 * line - 1:
                pass_up(c, kind)
    start_down()

    own_local[3].wait()
    own_local[5].wait()
    for source in (buddy, corner):
        arrived(wo, wo_recv, source).wait_recv()
        arrived(att, att_recv, source).wait_recv()
    tile = tok // 4
    piece = 512

    def mix(i, carry):
        rows = pl.ds(pl.multiple_of(i * tile, tile), tile)
        squares = jnp.zeros((tile, 1), F32)
        for c in range(0, width, piece):
            acc = jnp.zeros((tile, piece), F32)
            for k in range(tp):
                term = jnp.dot(
                    att[k, rows, :], wo[k, :, pl.ds(c, piece)], preferred_element_type=F32
                )
                acc = acc + term.astype(BF16).astype(F32)
            new = (mid[rows, pl.ds(c, piece)].astype(F32) + acc).astype(BF16)
            mid[rows, pl.ds(c, piece)] = new
            wide = new.astype(F32)
            squares = squares + jnp.sum(wide * wide, axis=-1, keepdims=True)
        scale = lax.rsqrt(squares * (1.0 / width) + EPS)
        for c in range(0, width, piece):
            wide = mid[rows, pl.ds(c, piece)].astype(F32)
            normed[rows, pl.ds(c, piece)] = (
                wide * scale * gain_ref[:, pl.ds(c, piece)]
            ).astype(BF16)
        return carry

    lax.fori_loop(0, 4, mix, 0)

    for c in range(5, 2 * line - 1):
        for kind in range(PIECES):
            pass_up(c, kind)
    lax.fori_loop(1, 3, pass_down, 0)

    for kind in range(2):
        own_local[kind].wait()

    def take_up(c, carry):
        there, valid, above = candidate(c)

        @pl.when(valid)
        def _():
            other = there * PAIR + (1 - side)
            for kind in range(PIECES):
                if kind < HALVES:
                    pl.when(c > 0)(up_copy(kind, other, 2).wait_recv)
                else:
                    up_copy(kind, other, 2).wait_recv()

        return carry

    lax.fori_loop(0, 2 * line - 1, take_up, 0)

    def project(i, carry):
        base = pl.multiple_of(i * tile, tile)
        left = normed[pl.ds(base, tile), :]
        rows = pl.ds(pl.multiple_of(base + EDGE, EDGE), tile)
        for weight, dest in ((wg, upg), (wv, upv)):
            for c in range(0, hid, piece):
                term = jnp.dot(left, weight[:, pl.ds(c, piece)], preferred_element_type=F32)
                dest[rows, pl.ds(c, piece)] = term.astype(BF16).astype(F32)
        return carry

    lax.fori_loop(0, 4, project, 0)

    def edge_low(kind):
        ref = (upg, upv)[kind]
        return remote(
            ref.at[pl.ds(EDGE, EDGE), :],
            ref.at[pl.ds(EDGE + tok, EDGE), :],
            edge_send.at[0, kind],
            edge_recv.at[1, kind],
            sp=me - 1,
        )

    def edge_high(kind):
        ref = (upg, upv)[kind]
        return remote(
            ref.at[pl.ds(tok, EDGE), :],
            ref.at[pl.ds(0, EDGE), :],
            edge_send.at[1, kind],
            edge_recv.at[0, kind],
            sp=me + 1,
        )

    none = jnp.zeros((EDGE, hid), F32)
    lax.fori_loop(3, min(5, 2 * line - 1), pass_down, 0)
    for kind in range(2):
        pl.when(has_low)(edge_low(kind).start)
        pl.when(has_high)(edge_high(kind).start)

    @pl.when(jnp.logical_not(has_low))
    def _():
        upg[pl.ds(0, EDGE), :] = none
        upv[pl.ds(0, EDGE), :] = none

    @pl.when(jnp.logical_not(has_high))
    def _():
        upg[pl.ds(EDGE + tok, EDGE), :] = none
        upv[pl.ds(EDGE + tok, EDGE), :] = none

    for kind in range(2):
        pl.when(has_low)(edge_high(kind).wait_recv)
        pl.when(has_high)(edge_low(kind).wait_recv)

    def gate(i, carry):
        base = pl.multiple_of(i * WINDOW, WINDOW)
        for c in range(0, hid, 256):
            lanes = pl.ds(c, 256)

            def convolve(ref, taps):
                field = ref[pl.ds(base, WINDOW + 2 * EDGE), lanes]
                taps = taps[:, lanes].astype(F32)
                return (
                    field[EDGE - 1 : EDGE - 1 + WINDOW] * taps[0:1]
                    + field[EDGE : EDGE + WINDOW] * taps[1:2]
                    + field[EDGE + 1 : EDGE + 1 + WINDOW] * taps[2:3]
                )

            g = convolve(upg, tg_ref)
            v = convolve(upv, tv_ref)
            hidden[pl.ds(base, WINDOW), lanes] = (g / (1.0 + jnp.exp(-g)) * v).astype(BF16)
        return carry

    lax.fori_loop(0, tok // WINDOW, gate, 0)

    def rows_of(owner):
        return pl.ds(pl.multiple_of(owner * share, share), share)

    def near_copy(block, k):
        return remote(
            terms.at[block, rows_of((buddy, corner)[k]), :],
            near.at[k, block],
            near_send.at[block, k],
            near_recv.at[block, k],
            tp=buddy,
        )

    def far_copy(block):
        return remote(
            pair_sum.at[block], far.at[block], far_send.at[block], far_recv.at[block], tp=across
        )

    def pass_pair(block):
        near_copy(block, 1).wait_recv()
        both = terms[block, rows_of(across), :].astype(F32) + near[1, block].astype(F32)
        pair_sum[block] = both.astype(BF16)
        far_copy(block).start()

    def process(block):
        def part(i, carry):
            rows = pl.ds(pl.multiple_of(i * tile, tile), tile)
            terms[block, rows, :] = jnp.dot(
                hidden[rows, :], wd[block], preferred_element_type=F32
            ).astype(BF16)
            return carry

        lax.fori_loop(0, 4, part, 0)
        near_copy(block, 1).start()
        near_copy(block, 0).start()

    own_local[2].wait()

    def down(c, carry):
        there, valid, above = candidate(c)
        block = there * PAIR + side

        @pl.when(valid)
        def _():
            @pl.when(c > 4)
            def _():
                pass_down(c, 0)

            process(block)

        before, was_valid, _ = candidate(jnp.maximum(c - 1, 0))

        @pl.when(was_valid & (c > 0))
        def _():
            other = before * PAIR + (1 - side)
            dn_copy(other, 2).wait_recv()
            process(other)
            pass_pair(before * PAIR + side)

        earlier, was_valid, _ = candidate(jnp.maximum(c - 2, 0))

        @pl.when(was_valid & (c > 1))
        def _():
            pass_pair(earlier * PAIR + (1 - side))

        return carry

    lax.fori_loop(0, 2 * line + 1, down, 0)

    my_rows = pl.ds(pl.multiple_of(my_tp * share, share), share)

    for block in range(sp):
        lanes = pl.ds(block * cols, cols)
        acc = mid[my_rows, lanes].astype(F32) + terms[block, my_rows, :].astype(F32)
        near_copy(block, 0).wait_recv()
        far_copy(block).wait_recv()
        acc = acc + near[0, block].astype(F32) + far[block].astype(F32)
        out_ref[:, lanes] = acc.astype(BF16)

    def drain(c, carry):
        there, valid, above = candidate(c)
        block = there * PAIR + side
        goes_down = can_down & (above | (c == 0))
        goes_up = can_up & (jnp.logical_not(above) | (c == 0))

        @pl.when(valid)
        def _():
            direct = (distance_of(there) > 1) | (c == 0)
            for kind in range(PIECES + 1):
                if kind < PIECES:
                    copy = functools.partial(up_copy, kind, block)
                else:
                    copy = functools.partial(dn_copy, block)
                pl.when(direct | (kind >= HALVES))(copy(2).wait_send)
                pl.when(goes_down)(copy(0).wait_send)
                pl.when(goes_up)(copy(1).wait_send)

        return carry

    for kind in range(HALVES):
        pl.when(can_down)(up_copy(kind, mate, 0).wait_send)
        pl.when(can_up)(up_copy(kind, mate, 1).wait_send)
    lax.fori_loop(0, 2 * line - 1, drain, 0)
    for k in range(tp - 1):
        wo_copy(k, k < 2).wait_send()
        att_copy(k).wait_send()
    pl.when(has_low)(kv_low.wait_send)
    pl.when(has_high)(kv_high.wait_send)
    for kind in range(2):
        pl.when(has_low)(edge_low(kind).wait_send)
        pl.when(has_high)(edge_high(kind).wait_send)

    def drain_rs(block, carry):
        near_copy(block, 0).wait_send()
        near_copy(block, 1).wait_send()
        far_copy(block).wait_send()
        return carry

    lax.fori_loop(0, sp, drain_rs, 0)


def kernel_shards(
    sp,
    tp,
    residual,
    query,
    key,
    value,
    sink,
    norm_gain,
    w_out,
    w_gate,
    w_value,
    conv_gate,
    conv_value,
    w_down,
):
    tok, width = residual.shape
    depth, hid = w_gate.shape
    cols = w_down.shape[1]
    heads = query.shape[1] // HD
    share = tok // tp
    offset = lax.axis_index("sp") * tok
    band = jnp.concatenate([key, value], axis=1)
    inverse = THETA ** (-(np.arange(2 * HD) % (HD // 2)) * 2.0 / HD)
    angle = (np.arange(tok + 2 * WINDOW) - WINDOW)[:, None] * inverse[None, :]
    first = offset.astype(F32) * jnp.asarray(inverse, F32)
    base = jnp.stack([jnp.cos(first), jnp.sin(first)])
    vmem = pl.BlockSpec(memory_space=pltpu.VMEM)
    smem = pl.BlockSpec(memory_space=pltpu.SMEM)
    anywhere = pl.BlockSpec(memory_space=pl.ANY)
    dma = pltpu.SemaphoreType.DMA
    return pl.pallas_call(
        functools.partial(layer_kernel, sp, tp),
        out_shape=jax.ShapeDtypeStruct((tok // tp, width), BF16),
        in_specs=[vmem] * 5 + [smem, anywhere, vmem] + [anywhere] * 3 + [vmem] * 2 + [anywhere],
        out_specs=vmem,
        scratch_shapes=[
            pltpu.VMEM((tok + 2 * WINDOW, 2 * HD), BF16),
            pltpu.VMEM((tok + 2 * WINDOW, 2 * HD), BF16),
            pltpu.VMEM((tok + 2 * WINDOW, 2 * HD), BF16),
            pltpu.VMEM((tp, tok, heads * HD), BF16),
            pltpu.VMEM((tp,) + w_out.shape, BF16),
            pltpu.VMEM((sp * depth, hid), BF16),
            pltpu.VMEM((sp * depth, hid), BF16),
            pltpu.VMEM((sp, hid, cols), BF16),
            pltpu.VMEM((tok, width), BF16),
            pltpu.VMEM((tok, width), BF16),
            pltpu.VMEM((tok + 2 * EDGE, hid), F32),
            pltpu.VMEM((tok + 2 * EDGE, hid), F32),
            pltpu.VMEM((tok, hid), BF16),
            pltpu.VMEM((sp, tok, cols), BF16),
            pltpu.VMEM((2, sp, share, cols), BF16),
            pltpu.VMEM((sp, share, cols), BF16),
            pltpu.VMEM((sp, share, cols), BF16),
            dma((6,)),
            dma((PIECES, sp, 3)),
            dma((PIECES, sp)),
            dma((sp, 3)),
            dma((sp,)),
            dma((tp - 1,)),
            dma((tp,)),
            dma((tp - 1,)),
            dma((tp,)),
            dma((2,)),
            dma((2,)),
            dma((2, 2)),
            dma((2, 2)),
            dma((sp, 2)),
            dma((sp, 2)),
            dma((sp,)),
            dma((sp,)),
        ],
        compiler_params=pltpu.CompilerParams(
            collective_id=0, has_side_effects=True, vmem_limit_bytes=66 * 1000 * 1000
        ),
        name="layer",
    )(
        query,
        band,
        jnp.asarray(np.cos(angle), F32),
        jnp.asarray(np.sin(angle), F32),
        base,
        sink,
        residual,
        norm_gain.reshape(1, -1),
        w_out,
        w_gate,
        w_value,
        conv_gate,
        conv_value,
        w_down,
    )


def solution(mesh):
    sp, tp = mesh.shape["sp"], mesh.shape["tp"]

    def shards(*args):
        if args[11].shape[1] % 128 or sp % PAIR or tp != 4 or args[2].shape[1] != HD:
            return plain_shards(*args)
        return kernel_shards(sp, tp, *args)

    return jax.shard_map(
        shards,
        mesh=mesh,
        in_specs=(
            P("sp", None),
            P("sp", "tp"),
            P("sp", "tp"),
            P("sp", "tp"),
            P("tp"),
            P(),
            P("tp", None),
            P("sp", "tp"),
            P("sp", "tp"),
            P(None, "tp"),
            P(None, "tp"),
            P("tp", "sp"),
        ),
        out_specs=P(("sp", "tp"), None),
        check_vma=False,
    )
```
